512 devices in a mesh: dp: 4 (over x), kv: 64 (over z, y), tp: 2 (over core).
Axes of the slice: x: 4, y: 8, z: 8, core: 2. Of those that a mesh axis runs over, the one named last changes fastest.
Arguments:
- tokens: bfloat16 [64, 16, 2048], P('dp', None, ('kv', 'tp')), may hold values from -190 to 190
- gain_in: float32 [2048], P(('kv', 'tp')), may hold values from 0.1 to 1.9
- w_qdown: bfloat16 [2048, 512], P(('kv', 'tp')), may hold values from -0.125 to 0.125
- w_kvdown: bfloat16 [2048, 256], P(('kv', 'tp')), may hold values from -0.125 to 0.125
- w_ropek: bfloat16 [2048, 32], replicated, may hold values from -0.125 to 0.125
- gain_qlat: float32 [512], replicated, may hold values from 0.1 to 1.9
- gain_kvlat: float32 [256], replicated, may hold values from 0.1 to 1.9
- w_qup: bfloat16 [512, 16, 96], P(None, 'tp'), may hold values from -0.25 to 0.25
- gain_q: float32 [96], replicated, may hold values from 0.4 to 20
- w_ukey: bfloat16 [256, 16, 64], P(None, 'tp'), may hold values from -0.75 to 0.75
- w_uval: bfloat16 [256, 16, 128], P(None, 'tp'), may hold values from -0.375 to 0.375
- w_out: bfloat16 [2048, 2048], P('tp', 'kv'), may hold values from -2.5 to 2.5
- gain_out: float32 [2048], P(('kv', 'tp')), may hold values from 0.1 to 1.9
- cache_lat: bfloat16 [64, 16384, 256], P('dp', 'kv'), may hold values from -6 to 6
- cache_rope: bfloat16 [64, 32, 16384], P('dp', None, 'kv'), may hold values from -6 to 6
- parents: int32 [64, 16], P('dp'), may hold values from -1 to 14, as said below
- lengths: int32 [64], P('dp'), may hold values from 8192 to 16352
- accepted: int32 [64], P('dp'), may hold values from 0 to 16
Outputs:
- attn_out: bfloat16 [64, 16, 2048], P('dp', None, ('kv', 'tp'))
- lat_cache_out: bfloat16 [64, 16384, 256], P('dp', 'kv')
- rope_cache_out: bfloat16 [64, 32, 16384], P('dp', None, 'kv')
The draws below stay inside these ranges and needn't reach their ends.
Inputs may be any that keep to these rules, and one draw needn't show every extreme that they name: `parents`: proposal j's parent is -1 (the last accepted token) or a proposal before j. Rows 0 .. lengths + accepted - 1 of a sequence's cache hold its past; the 16 positions after them lie inside the cache.
All inputs are finite; a program needn't handle non-finite values.
Results may differ from the reference program's by a relative error of at most 0.0102.
The reference program's roundings to bfloat16 on the way count: a program that leaves them out, or rounds other values in their place, can miss the bound.
Values may be sent and summed in bfloat16 or wider, within the bound.
No kernel may reach another device: no remote copies, remote signals or barrier semaphores. Data moves between devices by JAX's collectives and lax.ppermute only.
A program may use at most 64 MiB of HBM per device.

```python
import jax
import jax.numpy as jnp
from jax import lax

MODEL = 2048
HEADS = 16
QRANK = 512
KVRANK = 256
NOPE = 64
ROPE = 32
VHEAD = 128
PROPS = 16
QKHEAD = 96
SEQS = 64
POSITIONS = 16384


def draw_tokens(key, part):
    base_key, rough_key, row_key = jax.random.split(jax.random.fold_in(key, 11), 3)
    column = jnp.arange(MODEL, dtype=jnp.float32) / (MODEL - 1)
    ramp = jnp.exp(jnp.log(10.0) * column)
    rough = jax.random.uniform(rough_key, (MODEL,), jnp.float32, 0.5, 1.5)
    row_scale = jnp.exp(jax.random.uniform(row_key, (SEQS, PROPS, 1), jnp.float32, 0.0, jnp.log(10.0)))
    noise = jax.random.normal(base_key, (SEQS, PROPS, MODEL), jnp.float32)
    noise = jnp.clip(noise, -5.0, 5.0)
    return (noise * ramp * rough * row_scale / 4.0).astype(jnp.bfloat16)


def draw_gain_q(key, part):
    inner = jax.random.fold_in(key, 23)
    values = 1.0 + 0.18 * jnp.clip(jax.random.normal(inner, (QKHEAD,), jnp.float32), -3.0, 3.0)
    return values.astype(jnp.float32)


def draw_w_out(key, part):
    base_key, rough_key = jax.random.split(jax.random.fold_in(key, 37), 2)
    column = jnp.arange(MODEL, dtype=jnp.float32) / (MODEL - 1)
    ramp = jnp.exp(jnp.log(10.0) * column)
    rough = jax.random.uniform(rough_key, (MODEL,), jnp.float32, 0.5, 1.5)
    noise = jnp.clip(jax.random.normal(base_key, (HEADS * VHEAD, MODEL), jnp.float32), -5.0, 5.0)
    return (noise * ramp * rough / 30.0).astype(jnp.bfloat16)


def draw_parents(key, part):
    raw = jax.random.randint(jax.random.fold_in(key, 41), (SEQS, PROPS), 0, 1 << 20, dtype=jnp.int32)
    limit = jnp.arange(PROPS, dtype=jnp.int32) + 1
    return (raw % limit[None, :] - 1).astype(jnp.int32)


def plant(values, rng, least, high):
    longest = values.shape.index(max(values.shape))
    spots = []
    for shift in (0, 1):
        where = [jax.random.randint(jax.random.fold_in(rng, axis), (), 0, length) for axis, length in enumerate(values.shape)]
        where[longest] = (where[longest] + shift) % values.shape[longest]
        spots.append(tuple(where))
    return values.at[spots[0]].set(least).at[spots[1]].set(high)


def level_of(key, extent, cuts, low, high):
    factor_of, own = 1.0, jax.random.fold_in(key, 6)
    for dim, parts in cuts:
        draws = jnp.exp(jax.random.uniform(jax.random.fold_in(own, dim), (parts,), jnp.float32, low / len(cuts), high / len(cuts)))
        factor_of = factor_of * jnp.repeat(draws, extent[dim] // parts).reshape([-1 if axis == dim else 1 for axis in range(len(extent))])
    return factor_of


def centred(stream_key, shape, scale, most, pieces=(), held_as=jnp.bfloat16):
    level = level_of(stream_key, shape, pieces, -0.22, 0.18) if pieces else 1.0
    entries = jax.random.normal(stream_key, shape, jnp.float32) * scale * level
    return jnp.minimum(jnp.maximum(entries, -most), most).astype(held_as)


def setup_inputs(seed: int = 0) -> dict:
    streams_of = jax.random.split(jax.random.key(seed), 19)
    return {
        "tokens": draw_tokens(jax.random.fold_in(streams_of[18], 71), 0),
        "gain_in": jnp.clip(1.0 + 0.18 * jax.random.normal(streams_of[1], (MODEL,), jnp.float32), 0.1, 1.9),
        "w_qdown": centred(streams_of[2], (MODEL, QRANK), MODEL ** -0.5, 0.125, ((0, 128),)),
        "w_kvdown": centred(streams_of[3], (MODEL, KVRANK), MODEL ** -0.5, 0.125, ((0, 128),)),
        "w_ropek": centred(streams_of[4], (MODEL, ROPE), MODEL ** -0.5, 0.125),
        "gain_qlat": jnp.clip(1.0 + 0.18 * jax.random.normal(streams_of[5], (QRANK,), jnp.float32), 0.1, 1.9),
        "gain_kvlat": jnp.clip(1.0 + 0.18 * jax.random.normal(streams_of[6], (KVRANK,), jnp.float32), 0.1, 1.9),
        "w_qup": centred(streams_of[7], (QRANK, HEADS, QKHEAD), QRANK ** -0.5, 0.25, ((1, 2),)),
        "gain_q": draw_gain_q(jax.random.fold_in(streams_of[18], 71), 0),
        "w_ukey": centred(streams_of[9], (KVRANK, HEADS, NOPE), NOPE ** -0.5, 0.75, ((1, 2),)),
        "w_uval": centred(streams_of[10], (KVRANK, HEADS, VHEAD), KVRANK ** -0.5, 0.375, ((1, 2),)),
        "w_out": draw_w_out(jax.random.fold_in(streams_of[18], 71), 0),
        "gain_out": jnp.clip(1.0 + 0.18 * jax.random.normal(streams_of[12], (MODEL,), jnp.float32), 0.1, 1.9),
        "cache_lat": centred(streams_of[13], (SEQS, POSITIONS, KVRANK), 1.0, 6.0, ((0, 4), (1, 64))),
        "cache_rope": centred(streams_of[14], (SEQS, ROPE, POSITIONS), 1.0, 6.0, ((0, 4), (2, 64))),
        "parents": draw_parents(jax.random.fold_in(streams_of[18], 71), 0),
        "lengths": plant(jax.random.randint(streams_of[16], (SEQS,), POSITIONS // 2, POSITIONS - 2 * PROPS + 1), jax.random.fold_in(streams_of[16], 1), POSITIONS // 2, POSITIONS - 2 * PROPS).astype(jnp.int32),
        "accepted": plant(jax.random.randint(streams_of[17], (SEQS,), 0, PROPS + 1), jax.random.fold_in(streams_of[17], 1), 0, PROPS).astype(jnp.int32),
    }


epsilon = 1e-06

def normed(values, gain_vec):
    return values * lax.rsqrt(lax.optimization_barrier(jnp.mean(values * values, axis=-1, keepdims=True)) + epsilon) * gain_vec

def rope_angles(position, half_dim):
    frequency = 10000.0 ** (-(jnp.arange(half_dim, dtype=jnp.float32) * 2.0) / (2 * half_dim))
    return position.astype(jnp.float32)[..., None] * frequency

def ancestry(parents):
    proposals = parents.shape[-1]
    parent_link = (parents[..., :, None] == jnp.arange(proposals, dtype=jnp.int32)).astype(jnp.float32)
    identity = jnp.broadcast_to(jnp.eye(proposals, dtype=jnp.float32), parent_link.shape)

    def extend(iteration, state_pair):
        reaches, current = state_pair
        current = jnp.einsum('sij,sjk->sik', current, parent_link, precision=lax.Precision.HIGHEST)
        return (reaches + current, current)
    reaches, current = lax.fori_loop(0, proposals - 1, extend, (identity, identity))
    depths = (lax.optimization_barrier(jnp.sum(reaches, axis=-1)) - 1.0).astype(jnp.int32)
    return (reaches, depths)

def to_half(values):
    return lax.optimization_barrier(values.astype(jnp.bfloat16))

def place_rows(cache_row, new_rows, start_at):
    return lax.dynamic_update_slice(cache_row, new_rows, (start_at, start_at * 0))

def place_columns(cache_row, new_rows, start_at):
    return lax.dynamic_update_slice(cache_row, new_rows.T, (start_at * 0, start_at))

def reference(tokens, gain_in, w_qdown, w_kvdown, w_ropek, gain_qlat, gain_kvlat, w_qup, gain_q, w_ukey, w_uval, w_out, gain_out, cache_lat, cache_rope, parents, lengths, accepted):
    tok32 = tokens.astype(jnp.float32)
    scaled = to_half(tok32 * gain_in).astype(jnp.float32)
    squares = lax.optimization_barrier(jnp.sum(tok32 * tok32, axis=-1))
    rescale = lax.rsqrt(squares / MODEL + epsilon)[..., None]

    def project(weight):
        return jnp.einsum('spd,dk->spk', scaled, weight.astype(jnp.float32)) * rescale
    query_latent = to_half(normed(project(w_qdown), gain_qlat))
    new_latent = to_half(normed(project(w_kvdown), gain_kvlat))
    new_rope = to_half(project(w_ropek))
    reaches, depths = ancestry(parents)
    starts = lengths + accepted
    query_pos = starts[:, None] + depths
    half_dim = ROPE // 2
    queries = jnp.einsum('spr,rhd->sphd', query_latent.astype(jnp.float32), w_qup.astype(jnp.float32))
    queries = normed(queries, gain_q)
    query_nope = to_half(queries[..., :NOPE]).astype(jnp.float32)
    angles = rope_angles(query_pos, half_dim)[:, :, None, :]
    lower_half = queries[..., NOPE:NOPE + half_dim]
    upper_half = queries[..., NOPE + half_dim:]
    query_rot = to_half(jnp.concatenate([lower_half * jnp.cos(angles) - upper_half * jnp.sin(angles), upper_half * jnp.cos(angles) + lower_half * jnp.sin(angles)], axis=-1))
    query_lat = to_half(jnp.einsum('sphn,khn->sphk', query_nope, w_ukey.astype(jnp.float32)))
    lat_out = jax.vmap(place_rows)(cache_lat, new_latent, starts)
    rope_out = jax.vmap(place_columns)(cache_rope, new_rope, starts)

    def attend(item):
        lat_query, rot_query, lat_rows, rope_rows, start_at, reach_one, depth_one = item
        slots = jnp.arange(POSITIONS, dtype=jnp.int32)
        offset = slots - start_at
        inside = (offset >= 0) & (offset < PROPS)
        matches = offset[:, None] == jnp.arange(PROPS, dtype=jnp.int32)[None, :]
        key_pos = jnp.where(inside, start_at + lax.optimization_barrier(jnp.sum(jnp.where(matches, depth_one[None, :], 0), axis=-1)), slots)
        ancestor = jnp.einsum('ij,pj->ip', reach_one, matches.astype(jnp.float32), precision=lax.Precision.HIGHEST)
        visible = (offset < 0)[None, :] | (ancestor > 0.5)
        key_angles = rope_angles(key_pos, half_dim).T
        rope32 = rope_rows.astype(jnp.float32)
        key_low = rope32[:half_dim]
        key_high = rope32[half_dim:]
        key_rot = to_half(jnp.concatenate([key_low * jnp.cos(key_angles) - key_high * jnp.sin(key_angles), key_high * jnp.cos(key_angles) + key_low * jnp.sin(key_angles)], axis=0))
        lat32 = lat_rows.astype(jnp.float32)
        scores = (jnp.einsum('ihk,pk->ihp', lat_query.astype(jnp.float32), lat32) + jnp.einsum('ihr,rp->ihp', rot_query.astype(jnp.float32), key_rot.astype(jnp.float32))) * (NOPE + ROPE) ** (-0.5)
        masked = jnp.where(visible[:, None, :], scores, -jnp.inf)
        row_max = lax.optimization_barrier(jnp.max(masked, axis=-1, keepdims=True))
        weights32 = jnp.exp(masked - row_max)
        denominator = lax.optimization_barrier(jnp.sum(weights32, axis=-1))
        weights = to_half(weights32).astype(jnp.float32)
        numerator = jnp.einsum('ihp,pk->ihk', weights, lat32)
        return (numerator, denominator)
    numerators, denominators = lax.map(attend, (query_lat, query_rot, lat_out, rope_out, starts, reaches, depths))
    valued = jnp.einsum('sphk,khv->sphv', numerators, w_uval.astype(jnp.float32), precision=lax.Precision.HIGHEST)
    head_out = to_half(valued / denominators[..., None])
    head_rows = head_out.reshape(head_out.shape[0], PROPS, HEADS * VHEAD).astype(jnp.float32)
    mixed = jnp.einsum('spx,xd->spd', head_rows, w_out.astype(jnp.float32))
    result = normed(mixed, gain_out).astype(jnp.bfloat16)
    return (result, lat_out, rope_out)
```

```python
import jax
import jax.numpy as jnp
from jax import lax
from jax.sharding import Mesh
from jax.sharding import PartitionSpec as P

KV_TP = ("kv_0", "kv_1", "tp")
KV = ("kv_0", "kv_1")

epsilon = 1e-06
F32 = jnp.float32
BF16 = jnp.bfloat16


def exchange(parts, axes):
    return lax.all_to_all(parts, axes, split_axis=0, concat_axis=0, tiled=True)


def from_everyone(shard, axes):
    return exchange(jnp.broadcast_to(shard[None], (lax.axis_size(axes), *shard.shape)), axes)


def bf16_terms(values, count):
    terms = []
    for _ in range(count):
        term = lax.reduce_precision(values, 8, 7)
        terms.append(term.astype(BF16))
        values = values - term
    return terms


def normed(values, gain_vec):
    return (
        values * lax.rsqrt(jnp.mean(values * values, axis=-1, keepdims=True) + epsilon) * gain_vec
    )


def rope_angles(position, half_dim):
    frequency = 10000.0 ** (-(jnp.arange(half_dim, dtype=jnp.float32) * 2.0) / (2 * half_dim))
    return position.astype(jnp.float32)[..., None] * frequency


def ancestry(parents):
    proposals = parents.shape[-1]
    step = (parents[..., :, None] == jnp.arange(proposals, dtype=jnp.int32)).astype(BF16)
    reaches = step + jnp.eye(proposals, dtype=BF16)
    covered = 2
    while covered < proposals:
        step = jnp.einsum("sij,sjk->sik", step, step, preferred_element_type=F32).astype(BF16)
        reaches = reaches + jnp.einsum(
            "sij,sjk->sik", reaches, step, preferred_element_type=F32
        ).astype(BF16)
        covered *= 2
    reaches = reaches.astype(F32)
    depths = (jnp.sum(reaches, axis=-1) - 1.0).astype(jnp.int32)
    return (reaches, depths)


def local(
    tokens,
    gain_in,
    w_qdown,
    w_kvdown,
    w_ropek,
    gain_qlat,
    gain_kvlat,
    w_qup,
    gain_q,
    w_ukey,
    w_uval,
    w_out,
    gain_out,
    cache_lat,
    cache_rope,
    parents,
    lengths,
    accepted,
):
    seq_count, proposals, local_width = tokens.shape
    rows = seq_count * proposals
    owners = lax.axis_size(KV)
    full_width = local_width * lax.axis_size(KV_TP)
    qrank, heads_here, qkhead = w_qup.shape
    kvrank, _, nope_dim = w_ukey.shape
    vhead = w_uval.shape[2]
    rope_dim = cache_rope.shape[1]
    half_dim = rope_dim // 2
    width = qrank + kvrank + rope_dim

    rope_rows = lax.dynamic_slice_in_dim(
        w_ropek, lax.axis_index(KV_TP) * local_width, local_width, 0
    )
    joined = jnp.concatenate([w_qdown, w_kvdown, rope_rows], axis=1)
    half = rows // lax.axis_size("tp")
    pair_tokens, pair_gain, pair_weights = lax.all_gather(
        (tokens.reshape(rows, local_width), gain_in[None], joined), "tp"
    )
    pair_tokens = lax.dynamic_slice_in_dim(pair_tokens, lax.axis_index("tp") * half, half, 1)
    tok_rows = pair_tokens.astype(F32)
    scaled = (tok_rows * pair_gain).astype(BF16)
    squares = jnp.sum(tok_rows * tok_rows, axis=(0, 2))
    partial_rows = jnp.einsum("crd,cdk->rk", scaled, pair_weights, preferred_element_type=F32)
    sent = jnp.concatenate([partial_rows, squares[:, None]], axis=1)
    arrived = exchange(sent.reshape(owners, half // owners, width + 1), KV)
    summed = arrived.sum(axis=0)
    latent_rows = summed[:, :width] * lax.rsqrt(summed[:, width] / full_width + epsilon)[:, None]
    share = jnp.concatenate(
        [
            normed(latent_rows[:, :qrank], gain_qlat).astype(BF16),
            normed(latent_rows[:, qrank : qrank + kvrank], gain_kvlat).astype(BF16),
            latent_rows[:, qrank + kvrank :].astype(BF16),
        ],
        axis=1,
    )
    everyone = from_everyone(share, KV).reshape(half, width)
    everyone = lax.all_gather(everyone, "tp", axis=0, tiled=True)
    query_latent = everyone[:, :qrank]
    new_latent = everyone[:, qrank : qrank + kvrank]
    new_rope = everyone[:, qrank + kvrank :]
    reaches, depths = ancestry(parents)
    starts = lengths + accepted
    query_pos = starts[:, None] + depths
    queries = jnp.dot(
        query_latent, w_qup.reshape(qrank, heads_here * qkhead), preferred_element_type=jnp.float32
    )
    queries = normed(queries.reshape(seq_count, proposals, heads_here, qkhead), gain_q)
    query_nope = queries[..., :nope_dim].astype(jnp.bfloat16)
    angles = rope_angles(query_pos, half_dim)[:, :, None, :]
    cosine = jnp.cos(angles)
    sines = jnp.sin(angles)
    lower_half = queries[..., nope_dim : nope_dim + half_dim]
    upper_half = queries[..., nope_dim + half_dim :]
    query_rot = jnp.concatenate(
        [lower_half * cosine - upper_half * sines, upper_half * cosine + lower_half * sines],
        axis=-1,
    ).astype(jnp.bfloat16)
    query_lat = jnp.einsum(
        "sihn,khn->sihk", query_nope, w_ukey, preferred_element_type=jnp.float32
    ).astype(jnp.bfloat16)
    pos_count = cache_lat.shape[1]
    slots = lax.axis_index(KV) * pos_count + jnp.arange(pos_count, dtype=jnp.int32)
    offset = slots[None, :] - starts[:, None]
    inside = (offset >= 0) & (offset < proposals)
    matches = offset[:, :, None] == jnp.arange(proposals, dtype=jnp.int32)
    selector = matches.astype(jnp.bfloat16)
    new_latent = new_latent.reshape(seq_count, proposals, kvrank)
    new_rope = new_rope.reshape(seq_count, proposals, rope_dim)
    placed = jnp.einsum(
        "spj,sjk->spk", selector, new_latent, preferred_element_type=jnp.float32
    ).astype(jnp.bfloat16)
    lat_out = jnp.where(inside[:, :, None], placed, cache_lat)
    placed_rope = jnp.einsum(
        "spj,sjr->srp", selector, new_rope, preferred_element_type=jnp.float32
    ).astype(jnp.bfloat16)
    rope_out = jnp.where(inside[:, None, :], placed_rope, cache_rope)
    key_pos = jnp.where(
        inside,
        starts[:, None] + jnp.sum(jnp.where(matches, depths[:, None, :], 0), axis=-1),
        slots[None, :],
    )
    ancestor = jnp.einsum(
        "sij,spj->sip", reaches, matches.astype(jnp.float32), precision=lax.Precision.HIGHEST
    )
    visible = (offset < 0)[:, None, :] | (ancestor > 0.5)
    key_angles = jnp.swapaxes(rope_angles(key_pos, half_dim), 1, 2)
    key_cos = jnp.cos(key_angles)
    key_sin = jnp.sin(key_angles)
    rope32 = rope_out.astype(jnp.float32)
    key_low = rope32[:, :half_dim, :]
    key_high = rope32[:, half_dim:, :]
    key_rot = jnp.concatenate(
        [key_low * key_cos - key_high * key_sin, key_high * key_cos + key_low * key_sin], axis=1
    ).astype(jnp.bfloat16)
    scores = (
        jnp.einsum("sihk,spk->sihp", query_lat, lat_out, preferred_element_type=jnp.float32)
        + jnp.einsum("sihr,srp->sihp", query_rot, key_rot, preferred_element_type=jnp.float32)
    ) * qkhead ** (-0.5)
    masked = jnp.where(visible[:, :, None, :], scores, -jnp.inf)
    row_max = jnp.maximum(jnp.max(masked, axis=-1), -1e30)
    weights32 = jnp.exp(masked - row_max[..., None])
    denominator = jnp.sum(weights32, axis=-1)
    weights = weights32.astype(BF16)
    numerator = jnp.einsum("sihp,spk->sihk", weights, lat_out, preferred_element_type=F32)
    numer_values = jnp.einsum(
        "...hk,khv->...hv", numerator, w_uval.astype(F32), precision=lax.Precision.HIGHEST
    )
    value_width = heads_here * vhead
    sent = jnp.concatenate(
        [
            numer_values.reshape(rows, value_width).astype(BF16),
            *(t.reshape(rows, heads_here) for t in bf16_terms(row_max, 3)),
            *(t.reshape(rows, heads_here) for t in bf16_terms(denominator, 3)),
        ],
        axis=1,
    )
    arrived = exchange(sent.reshape(owners, rows // owners, sent.shape[1]), KV).astype(F32)
    extras = arrived[..., value_width:].reshape(owners, rows // owners, 2, 3, heads_here).sum(3)
    maxima = extras[:, :, 0]
    factor = jnp.exp(maxima - jnp.max(maxima, axis=0))
    denom_all = jnp.sum(factor * extras[:, :, 1], axis=0)
    values_all = jnp.sum(
        factor[..., None] * arrived[..., :value_width].reshape(*factor.shape, vhead), axis=0
    )
    head_share = (values_all / denom_all[..., None]).astype(BF16)
    head_rows = from_everyone(head_share.reshape(rows // owners, value_width), KV)
    partial_out = jnp.dot(
        head_rows.reshape(rows, value_width), w_out, preferred_element_type=F32
    )
    mixed = lax.all_gather(partial_out, "tp").sum(axis=0)
    local_squares = jnp.sum(mixed * mixed, axis=-1)
    norm_total = from_everyone(local_squares[None], KV).sum(axis=(0, 1))
    own = lax.dynamic_slice_in_dim(mixed, lax.axis_index("tp") * local_width, local_width, 1)
    result = own * lax.rsqrt(norm_total / full_width + epsilon)[:, None] * gain_out
    result = result.astype(BF16).reshape(seq_count, proposals, local_width)
    return (result, lat_out, rope_out)


def solution(mesh):
    torus = Mesh(
        mesh.devices.reshape(mesh.shape["dp"], 8, 8, mesh.shape["tp"]), ("dp", "kv_0", "kv_1", "tp")
    )
    return jax.shard_map(
        local,
        mesh=torus,
        in_specs=(
            P("dp", None, KV_TP),
            P(KV_TP),
            P(KV_TP, None),
            P(KV_TP, None),
            P(),
            P(),
            P(),
            P(None, "tp", None),
            P(),
            P(None, "tp", None),
            P(None, "tp", None),
            P("tp", KV),
            P(KV_TP),
            P("dp", KV, None),
            P("dp", None, KV),
            P("dp", None),
            P("dp"),
            P("dp"),
        ),
        out_specs=(P("dp", None, KV_TP), P("dp", KV, None), P("dp", None, KV)),
        check_vma=False,
    )
```

```python
import jax
import jax.numpy as jnp
from jax import lax
from jax.experimental import pallas as pl
from jax.experimental.pallas import tpu as pltpu
from jax.sharding import Mesh
from jax.sharding import PartitionSpec as P

KV_TP = ("kv_0", "kv_1", "tp")
KV = ("kv_0", "kv_1")

epsilon = 1e-06
F32 = jnp.float32
BF16 = jnp.bfloat16
LOWEST = -1e30
HIDDEN = -3e38


def exchange(parts, axes):
    return lax.all_to_all(parts, axes, split_axis=0, concat_axis=0, tiled=True)


def from_everyone(shard, axes):
    return exchange(jnp.broadcast_to(shard[None], (lax.axis_size(axes), *shard.shape)), axes)


def normed(values, gain_vec):
    return (
        values * lax.rsqrt(jnp.mean(values * values, axis=-1, keepdims=True) + epsilon) * gain_vec
    )


def rope_angles(position, half_dim):
    frequency = 10000.0 ** (-(jnp.arange(half_dim, dtype=jnp.float32) * 2.0) / (2 * half_dim))
    return position.astype(jnp.float32)[..., None] * frequency


def ancestry(parents):
    proposals = parents.shape[-1]
    step = (parents[..., :, None] == jnp.arange(proposals, dtype=jnp.int32)).astype(BF16)
    reaches = step + jnp.eye(proposals, dtype=BF16)
    covered = 2
    while covered < proposals:
        step = jnp.einsum("sij,sjk->sik", step, step, preferred_element_type=F32).astype(BF16)
        reaches = reaches + jnp.einsum(
            "sij,sjk->sik", reaches, step, preferred_element_type=F32
        ).astype(BF16)
        covered *= 2
    reaches = reaches.astype(F32)
    depths = (jnp.sum(reaches, axis=-1) - 1.0).astype(jnp.int32)
    return (reaches, depths)


def attend_kernel(
    starts,
    base,
    lat_rows,
    w_query,
    gain,
    w_key,
    w_value,
    query_cos,
    query_sin,
    key_cos,
    key_sin,
    reach,
    cache_lat,
    cache_rope,
    lat_out,
    rope_out,
    sent,
    q_lat,
    q_rot,
    k_rot,
    bias,
    numer,
):
    step = pl.program_id(0)
    block, pos_count, kvrank = cache_lat.shape
    heads = w_key.shape[0]
    rope_dim = cache_rope.shape[1]
    half_dim = rope_dim // 2
    proposals = reach.shape[2]
    seq_count = q_lat.shape[0]
    qrank = w_query.shape[0]
    lanes = w_key.shape[1]
    qkhead = lanes - rope_dim
    scale = qkhead ** (-0.5)

    @pl.when(step == 0)
    def _():
        projected = jnp.dot(
            lat_rows[:, :qrank], w_query[...], preferred_element_type=F32
        )
        counted = lax.broadcasted_iota(jnp.int32, (1, lanes), 1) < qkhead
        for h in range(heads):
            one = projected[:, h * lanes : (h + 1) * lanes]
            mean = (
                jnp.sum(jnp.where(counted, one * one, 0.0), axis=1, keepdims=True) / qkhead
            )
            one = one * lax.rsqrt(mean + epsilon) * gain[...]
            at = pl.ds(h * proposals, proposals)
            moved = jnp.dot(one.astype(BF16), w_key[h], preferred_element_type=F32)
            q_lat[:, at, :] = moved.astype(BF16).reshape(seq_count, proposals, kvrank)
            turned = one * query_cos[...] + pltpu.roll(one, rope_dim, 1) * query_sin[...]
            q_rot[:, at, :] = turned.astype(BF16).reshape(seq_count, proposals, lanes)

    for j in range(block):
        s = step * block + j
        offset = base[0] - starts[s]
        rope32 = cache_rope[j].astype(F32)
        low, high = rope32[:half_dim], rope32[half_dim:]
        cosine, sine = key_cos[...], key_sin[...]
        k_rot[j, :half_dim] = (low * cosine - high * sine).astype(BF16)
        k_rot[j, half_dim:] = (high * cosine + low * sine).astype(BF16)
        hit = (offset > -pos_count) & (offset < proposals)

        @pl.when(jnp.logical_not(hit))
        def _():
            lat_out[j] = cache_lat[j]
            rope_out[j] = cache_rope[j]
            bias[j] = jnp.full(bias.shape[1:], jnp.where(offset < 0, 0.0, HIDDEN), F32)

        @pl.when(hit)
        def _():
            rows = pl.ds(pl.multiple_of(s * proposals, proposals), proposals)
            down = lax.broadcasted_iota(jnp.int32, (pos_count, proposals), 0) + offset
            picked = down == lax.broadcasted_iota(jnp.int32, (pos_count, proposals), 1)
            across = lax.broadcasted_iota(jnp.int32, (proposals, pos_count), 1) + offset
            chosen = across == lax.broadcasted_iota(jnp.int32, (proposals, pos_count), 0)
            chosen = chosen.astype(F32).astype(BF16)
            along = lax.broadcasted_iota(jnp.int32, (1, pos_count), 1) + offset
            inside = (along >= 0) & (along < proposals)
            beneath = lax.broadcasted_iota(jnp.int32, (pos_count, 1), 0) + offset
            placed = jnp.dot(
                picked.astype(F32).astype(BF16),
                lat_rows[rows, qrank : qrank + kvrank],
                preferred_element_type=F32,
            )
            lat_out[j] = jnp.where(
                (beneath >= 0) & (beneath < proposals), placed, cache_lat[j].astype(F32)
            ).astype(BF16)
            new_rope = lat_rows[rows, qrank + kvrank :].astype(F32)
            swapped = jnp.concatenate([new_rope[:, half_dim:], new_rope[:, :half_dim]], axis=1)
            turned = (
                new_rope * query_cos[rows, :rope_dim] + swapped * query_sin[rows, :rope_dim]
            )
            contract = (((0,), (0,)), ((), ()))
            put = lax.dot_general(
                new_rope.astype(BF16), chosen, contract, preferred_element_type=F32
            )
            rope_out[j] = jnp.where(inside, put, rope32).astype(BF16)
            put = lax.dot_general(
                turned.astype(BF16), chosen, contract, preferred_element_type=F32
            )
            k_rot[j] = jnp.where(inside, put, k_rot[j].astype(F32)).astype(BF16)
            seen = jnp.dot(reach[s], chosen, preferred_element_type=F32)
            bias[j] = jnp.where((seen > 0.5) | (along < 0), 0.0, HIDDEN)

    for j in range(block):
        s = step * block + j
        keys = lat_out[j]
        score = lax.dot_general(
            q_lat[s], keys, (((1,), (1,)), ((), ())), preferred_element_type=F32
        )
        score = score + jnp.dot(
            q_rot[s][:, :rope_dim], k_rot[j], preferred_element_type=F32
        )
        score = score * scale + bias[j]
        top = jnp.maximum(jnp.max(score, axis=1, keepdims=True), LOWEST)
        weights = jnp.exp(score - top)
        total = jnp.sum(weights, axis=1, keepdims=True)
        numer[j] = jnp.dot(weights.astype(BF16), keys, preferred_element_type=F32)
        lane = lax.broadcasted_iota(jnp.int32, (1, 128), 1)
        terms = jnp.zeros((heads * proposals, 128), F32)
        for first, rest in ((0, top), (3, total)):
            for k in range(3):
                term = rest.astype(BF16).astype(F32)
                terms = jnp.where(lane == first + k, term, terms)
                rest = rest - term
        extra = jnp.transpose(terms)[:8].astype(BF16)
        for c in range(heads // 2):
            sent[j * (heads // 2) + c, 2 * proposals :, :] = extra

    for h in range(heads):
        part = numer[:, pl.ds(h * proposals, proposals), :].reshape(block * proposals, kvrank)
        upper = part.astype(BF16)
        lower = (part - upper.astype(F32)).astype(BF16)
        both = jnp.dot(
            jnp.concatenate([upper, lower], axis=0), w_value[h], preferred_element_type=F32
        )
        value = (both[: block * proposals] + both[block * proposals :]).astype(BF16)
        for j in range(block):
            sent[
                j * (heads // 2) + h // 2,
                (h % 2) * proposals : (h % 2 + 1) * proposals,
                :,
            ] = value[j * proposals : (j + 1) * proposals]


def attend(starts, base, lat_rows, weights, tables, reach, cache_lat, cache_rope):
    w_query, gain, w_key, w_value = weights
    seq_count, pos_count, kvrank = cache_lat.shape
    rope_dim = cache_rope.shape[1]
    heads, lanes, _ = w_key.shape
    proposals = reach.shape[2]
    rows = heads * proposals
    block = 4
    whole = pl.BlockSpec(memory_space=pltpu.VMEM)
    smem = pl.BlockSpec(memory_space=pltpu.SMEM)
    lat_spec = pl.BlockSpec((block, pos_count, kvrank), lambda g: (g, 0, 0))
    rope_spec = pl.BlockSpec((block, rope_dim, pos_count), lambda g: (g, 0, 0))
    chunks = heads // 2
    sent_shape = (seq_count * chunks, 2 * proposals + 8, w_value.shape[2])
    return pl.pallas_call(
        attend_kernel,
        grid=(seq_count // block,),
        in_specs=[smem, smem, *[whole] * 10, lat_spec, rope_spec],
        out_specs=[
            lat_spec,
            rope_spec,
            pl.BlockSpec((block * chunks, *sent_shape[1:]), lambda g: (g, 0, 0)),
        ],
        out_shape=[
            jax.ShapeDtypeStruct(cache_lat.shape, BF16),
            jax.ShapeDtypeStruct(cache_rope.shape, BF16),
            jax.ShapeDtypeStruct(sent_shape, BF16),
        ],
        scratch_shapes=[
            pltpu.VMEM((seq_count, rows, kvrank), BF16),
            pltpu.VMEM((seq_count, rows, lanes), BF16),
            pltpu.VMEM((block, rope_dim, pos_count), BF16),
            pltpu.VMEM((block, rows, pos_count), F32),
            pltpu.VMEM((block, rows, kvrank), F32),
        ],
        compiler_params=pltpu.CompilerParams(vmem_limit_bytes=24 * 1024 * 1024),
        cost_estimate=pl.CostEstimate(
            flops=10**9, bytes_accessed=8 * 10**6, transcendentals=10**6
        ),
    )(starts, base, lat_rows, w_query, gain, w_key, w_value, *tables, reach, cache_lat, cache_rope)


def project_kernel(heads_in, w_out, result):
    seq_count, heads, proposals, vhead = heads_in.shape
    total = jnp.zeros(result.shape, F32)
    for h in range(heads):
        total += jnp.dot(
            heads_in[:, h].reshape(seq_count * proposals, vhead),
            w_out[h * vhead : (h + 1) * vhead, :],
            preferred_element_type=F32,
        )
    result[...] = total


def project(heads_in, w_out):
    seq_count, heads, proposals, vhead = heads_in.shape
    return pl.pallas_call(
        project_kernel,
        out_shape=jax.ShapeDtypeStruct((seq_count * proposals, w_out.shape[1]), F32),
        in_specs=[pl.BlockSpec(memory_space=pltpu.VMEM)] * 2,
        out_specs=pl.BlockSpec(memory_space=pltpu.VMEM),
        compiler_params=pltpu.CompilerParams(vmem_limit_bytes=8 * 1024 * 1024),
        cost_estimate=pl.CostEstimate(
            flops=2 * 10**7, bytes_accessed=6 * 10**5, transcendentals=0
        ),
    )(heads_in, w_out)


def local(
    tokens,
    gain_in,
    w_qdown,
    w_kvdown,
    w_ropek,
    gain_qlat,
    gain_kvlat,
    w_qup,
    gain_q,
    w_ukey,
    w_uval,
    w_out,
    gain_out,
    cache_lat,
    cache_rope,
    parents,
    lengths,
    accepted,
):
    seq_count, proposals, local_width = tokens.shape
    rows = seq_count * proposals
    owners = lax.axis_size(KV)
    full_width = local_width * lax.axis_size(KV_TP)
    qrank, heads_here, qkhead = w_qup.shape
    kvrank, _, nope_dim = w_ukey.shape
    vhead = w_uval.shape[2]
    rope_dim = cache_rope.shape[1]
    half_dim = rope_dim // 2
    width = qrank + kvrank + rope_dim

    rope_rows = lax.dynamic_slice_in_dim(
        w_ropek, lax.axis_index(KV_TP) * local_width, local_width, 0
    )
    joined = jnp.concatenate([w_qdown, w_kvdown, rope_rows], axis=1)
    half = rows // lax.axis_size("tp")
    pair_tokens, pair_gain, pair_weights = lax.all_gather(
        (tokens.reshape(rows, local_width), gain_in[None], joined), "tp"
    )
    pair_tokens = lax.dynamic_slice_in_dim(pair_tokens, lax.axis_index("tp") * half, half, 1)
    tok_rows = pair_tokens.astype(F32)
    scaled = (tok_rows * pair_gain).astype(BF16)
    squares = jnp.sum(tok_rows * tok_rows, axis=(0, 2))
    partial_rows = jnp.einsum("crd,cdk->rk", scaled, pair_weights, preferred_element_type=F32)
    sent = jnp.concatenate([partial_rows, squares[:, None]], axis=1)
    arrived = exchange(sent.reshape(owners, half // owners, width + 1), KV)
    summed = arrived.sum(axis=0)
    latent_rows = summed[:, :width] * lax.rsqrt(summed[:, width] / full_width + epsilon)[:, None]
    share = jnp.concatenate(
        [
            normed(latent_rows[:, :qrank], gain_qlat).astype(BF16),
            normed(latent_rows[:, qrank : qrank + kvrank], gain_kvlat).astype(BF16),
            latent_rows[:, qrank + kvrank :].astype(BF16),
        ],
        axis=1,
    )
    everyone = from_everyone(share, KV).reshape(half, width)
    everyone = lax.all_gather(everyone, "tp", axis=0, tiled=True)
    reaches, depths = ancestry(parents)
    starts = lengths + accepted
    angles = rope_angles(starts[:, None] + depths, half_dim).reshape(rows, half_dim)
    cosine, sine = jnp.cos(angles), jnp.sin(angles)
    lanes = qkhead + rope_dim
    spare = ((0, 0), (0, lanes - rope_dim))
    pos_count = cache_lat.shape[1]
    base = lax.axis_index(KV) * pos_count
    slot_angles = rope_angles(base + jnp.arange(pos_count, dtype=jnp.int32), half_dim).T
    tables = (
        jnp.pad(jnp.concatenate([cosine, cosine], axis=1), spare),
        jnp.pad(jnp.concatenate([-sine, sine], axis=1), spare),
        jnp.cos(slot_angles),
        jnp.sin(slot_angles),
    )

    def arranged(values):
        nope, low, high = jnp.split(values, [nope_dim, nope_dim + half_dim], axis=-1)
        return jnp.concatenate([low, high, nope, high, low], axis=-1)

    weights = (
        arranged(w_qup).reshape(qrank, heads_here * lanes),
        arranged(gain_q)[None],
        jnp.pad(jnp.transpose(w_ukey, (1, 2, 0)), ((0, 0), (rope_dim, rope_dim), (0, 0))),
        jnp.transpose(w_uval, (1, 0, 2)),
    )
    reach = jnp.tile(reaches.astype(BF16), (1, heads_here, 1))
    lat_out, rope_out, sent = attend(
        starts, base[None], everyone, weights, tables, reach, cache_lat, cache_rope
    )
    arrived = exchange(sent, KV).astype(F32)
    group = 2 * proposals
    chunk = lax.rem(lax.axis_index(KV), heads_here // 2)
    extras = lax.dynamic_slice_in_dim(arrived[:, group:], chunk * group, group, 2)
    maxima = extras[:, 0] + extras[:, 1] + extras[:, 2]
    denominators = extras[:, 3] + extras[:, 4] + extras[:, 5]
    factor = jnp.exp(maxima - jnp.max(maxima, axis=0))
    denom_all = jnp.sum(factor * denominators, axis=0)
    values_all = jnp.sum(factor[..., None] * arrived[:, :group], axis=0)
    head_share = (values_all / denom_all[:, None]).astype(BF16)
    head_rows = from_everyone(head_share, KV)
    partial_out = project(head_rows.reshape(seq_count, heads_here, proposals, vhead), w_out)
    mixed = lax.all_gather(partial_out, "tp").sum(axis=0)
    local_squares = jnp.sum(mixed * mixed, axis=-1)
    norm_total = from_everyone(local_squares[None], KV).sum(axis=(0, 1))
    own = lax.dynamic_slice_in_dim(mixed, lax.axis_index("tp") * local_width, local_width, 1)
    result = own * lax.rsqrt(norm_total / full_width + epsilon)[:, None] * gain_out
    result = result.astype(BF16).reshape(seq_count, proposals, local_width)
    return (result, lat_out, rope_out)


def solution(mesh):
    torus = Mesh(
        mesh.devices.reshape(mesh.shape["dp"], 8, 8, mesh.shape["tp"]), ("dp", "kv_0", "kv_1", "tp")
    )
    return jax.shard_map(
        local,
        mesh=torus,
        in_specs=(
            P("dp", None, KV_TP),
            P(KV_TP),
            P(KV_TP, None),
            P(KV_TP, None),
            P(),
            P(),
            P(),
            P(None, "tp", None),
            P(),
            P(None, "tp", None),
            P(None, "tp", None),
            P("tp", KV),
            P(KV_TP),
            P("dp", KV, None),
            P("dp", None, KV),
            P("dp", None),
            P("dp"),
            P("dp"),
        ),
        out_specs=(P("dp", None, KV_TP), P("dp", KV, None), P("dp", None, KV)),
        check_vma=False,
    )
```

```python
import functools

import jax
import jax.numpy as jnp
from jax import lax
from jax.experimental import pallas as pl
from jax.experimental.pallas import tpu as pltpu
from jax.sharding import Mesh
from jax.sharding import PartitionSpec as P

KV_TP = ("kv_0", "kv_1", "tp")
KV = ("kv_0", "kv_1")

epsilon = 1e-06
F32 = jnp.float32
BF16 = jnp.bfloat16
LOWEST = -1e30
HIDDEN = -3e38


def exchange(parts, axes):
    return lax.all_to_all(parts, axes, split_axis=0, concat_axis=0, tiled=True)


def from_everyone(shard, axes):
    return exchange(jnp.broadcast_to(shard[None], (lax.axis_size(axes), *shard.shape)), axes)


def normed(values, gain_vec):
    return (
        values * lax.rsqrt(jnp.mean(values * values, axis=-1, keepdims=True) + epsilon) * gain_vec
    )


def rope_angles(position, half_dim):
    frequency = 10000.0 ** (-(jnp.arange(half_dim, dtype=jnp.float32) * 2.0) / (2 * half_dim))
    return position.astype(jnp.float32)[..., None] * frequency


def ancestry(parents):
    proposals = parents.shape[-1]
    step = (parents[..., :, None] == jnp.arange(proposals, dtype=jnp.int32)).astype(BF16)
    reaches = step + jnp.eye(proposals, dtype=BF16)
    covered = 2
    while covered < proposals:
        step = jnp.einsum("sij,sjk->sik", step, step, preferred_element_type=F32).astype(BF16)
        reaches = reaches + jnp.einsum(
            "sij,sjk->sik", reaches, step, preferred_element_type=F32
        ).astype(BF16)
        covered *= 2
    reaches = reaches.astype(F32)
    depths = (jnp.sum(reaches, axis=-1) - 1.0).astype(jnp.int32)
    return (reaches, depths)


def gather_kernel(index, tokens, gain, w_qdown, w_kvdown, rope_columns, out):
    width = tokens.shape[2]
    rows = tokens.shape[0] * tokens.shape[1]
    qrank, kvrank = w_qdown.shape[1], w_kvdown.shape[1]
    rope_dim, lanes = rope_columns.shape
    tok_rows = tokens[...].astype(F32).reshape(rows, width)
    scaled = (tok_rows * gain[...]).astype(BF16).astype(F32)
    out[:width, :rows] = jnp.transpose(scaled).astype(BF16)
    out[:width, rows : rows + qrank] = w_qdown[...]
    out[:width, rows + qrank : rows + qrank + kvrank] = w_kvdown[...]
    at = rows + qrank + kvrank
    shift = lax.rem(lanes - lax.rem(index[0] * width, lanes), lanes)
    turned = pltpu.roll(rope_columns[...].astype(F32), shift, 1)
    padded = jnp.concatenate([turned, jnp.zeros((lanes - rope_dim, lanes), F32)], axis=0)
    out[:width, at:] = jnp.transpose(padded)[:width].astype(BF16)
    flipped = jnp.transpose(tok_rows)
    squares = jnp.sum(flipped * flipped, axis=0, keepdims=True)
    row = lax.broadcasted_iota(jnp.int32, (width, rows), 0)
    terms = jnp.zeros((width, rows), F32)
    for k in range(3):
        term = squares.astype(BF16).astype(F32)
        terms = jnp.where(row == k, term, terms)
        squares = squares - term
    out[width:, :rows] = terms.astype(BF16)
    out[width:, rows:at] = jnp.zeros((width, at - rows), BF16)
    row = lax.broadcasted_iota(jnp.int32, (width, lanes), 0)
    lane = lax.broadcasted_iota(jnp.int32, (width, lanes), 1)
    out[width:, at:] = jnp.where((row < 3) & (lane == rope_dim), 1.0, 0.0).astype(BF16)


def gather_inputs(index, tokens, gain_in, w_qdown, w_kvdown, w_ropek):
    width = tokens.shape[2]
    rows = tokens.shape[0] * tokens.shape[1]
    lanes = 128
    whole = pl.BlockSpec(memory_space=pltpu.VMEM)
    shape = (2 * width, rows + w_qdown.shape[1] + w_kvdown.shape[1] + lanes)
    return pl.pallas_call(
        gather_kernel,
        grid_spec=pltpu.PrefetchScalarGridSpec(
            num_scalar_prefetch=1,
            grid=(1,),
            in_specs=[
                *[whole] * 4,
                pl.BlockSpec(
                    (w_ropek.shape[1], lanes), lambda g, index: (0, index[0] * width // lanes)
                ),
            ],
            out_specs=whole,
        ),
        out_shape=jax.ShapeDtypeStruct(shape, BF16),
        cost_estimate=pl.CostEstimate(flops=10**5, bytes_accessed=10**5, transcendentals=0),
    )(index, tokens, gain_in[None], w_qdown, w_kvdown, w_ropek.T)


def latent_kernel(full_width, arrived, gain_qlat, gain_kvlat, out):
    qrank, kvrank = gain_qlat.shape[1], gain_kvlat.shape[1]
    summed = jnp.sum(arrived[...], axis=0)
    lanes = 128
    at = qrank + kvrank
    lane = lax.broadcasted_iota(jnp.int32, (1, lanes), 1)
    last = summed[:, at:]
    rope_dim = 32
    squares = jnp.sum(jnp.where(lane == rope_dim, last, 0.0), axis=1, keepdims=True)
    rescale = lax.rsqrt(squares / full_width + epsilon)
    share = jnp.concatenate(
        [
            normed(summed[:, :qrank] * rescale, gain_qlat[...]),
            normed(summed[:, qrank:at] * rescale, gain_kvlat[...]),
            jnp.where(lane < rope_dim, last * rescale, 0.0),
            jnp.zeros(last.shape, F32),
        ],
        axis=1,
    )
    pieces = [share[:, c * lanes : (c + 1) * lanes] for c in range(share.shape[1] // lanes)]
    stacked = jnp.concatenate(pieces, axis=0).astype(BF16)
    out[...] = jnp.broadcast_to(stacked[None], out.shape)


def latents(arrived, full_width, gain_qlat, gain_kvlat):
    owners = arrived.shape[0]
    return pl.pallas_call(
        functools.partial(latent_kernel, full_width),
        in_specs=[pl.BlockSpec(memory_space=pltpu.VMEM)] * 3,
        out_specs=pl.BlockSpec(memory_space=pltpu.VMEM),
        out_shape=jax.ShapeDtypeStruct((owners, 16, 128), BF16),
        compiler_params=pltpu.CompilerParams(vmem_limit_bytes=8 * 1024 * 1024),
        cost_estimate=pl.CostEstimate(flops=10**5, bytes_accessed=10**6, transcendentals=0),
    )(arrived, gain_qlat[None], gain_kvlat[None])


def attend_kernel(
    starts,
    base,
    packed,
    w_query,
    gain,
    w_key,
    w_value,
    query_cos,
    query_sin,
    key_cos,
    key_sin,
    reach,
    cache_lat,
    cache_rope,
    lat_out,
    rope_out,
    sent,
    q_lat,
    q_rot,
    k_rot,
    bias,
    numer,
    lat_rows,
):
    step = pl.program_id(0)
    block, pos_count, kvrank = cache_lat.shape
    heads = w_key.shape[0]
    rope_dim = cache_rope.shape[1]
    half_dim = rope_dim // 2
    proposals = reach.shape[2]
    seq_count = q_lat.shape[0]
    qrank = w_query.shape[0]
    lanes = w_key.shape[1]
    qkhead = lanes - rope_dim
    scale = qkhead ** (-0.5)

    @pl.when(step == 0)
    def _():
        for c in range(lat_rows.shape[1] // 128):
            piece = packed[:, 2 * c : 2 * c + 2, :]
            lat_rows[:, c * 128 : (c + 1) * 128] = piece.reshape(lat_rows.shape[0], 128)
        projected = jnp.dot(
            lat_rows[:, :qrank], w_query[...], preferred_element_type=F32
        )
        counted = lax.broadcasted_iota(jnp.int32, (1, lanes), 1) < qkhead
        for h in range(heads):
            one = projected[:, h * lanes : (h + 1) * lanes]
            mean = (
                jnp.sum(jnp.where(counted, one * one, 0.0), axis=1, keepdims=True) / qkhead
            )
            one = one * lax.rsqrt(mean + epsilon) * gain[...]
            at = pl.ds(h * proposals, proposals)
            moved = jnp.dot(one.astype(BF16), w_key[h], preferred_element_type=F32)
            q_lat[:, at, :] = moved.astype(BF16).reshape(seq_count, proposals, kvrank)
            turned = one * query_cos[...] + pltpu.roll(one, rope_dim, 1) * query_sin[...]
            q_rot[:, at, :] = turned.astype(BF16).reshape(seq_count, proposals, lanes)

    for j in range(block):
        s = step * block + j
        offset = base[0] - starts[s]
        rope32 = cache_rope[j].astype(F32)
        low, high = rope32[:half_dim], rope32[half_dim:]
        cosine, sine = key_cos[...], key_sin[...]
        k_rot[j, :half_dim] = (low * cosine - high * sine).astype(BF16)
        k_rot[j, half_dim:] = (high * cosine + low * sine).astype(BF16)
        hit = (offset > -pos_count) & (offset < proposals)

        @pl.when(jnp.logical_not(hit))
        def _():
            lat_out[j] = cache_lat[j]
            rope_out[j] = cache_rope[j]
            bias[j] = jnp.full(bias.shape[1:], jnp.where(offset < 0, 0.0, HIDDEN), F32)

        @pl.when(hit)
        def _():
            rows = pl.ds(pl.multiple_of(s * proposals, proposals), proposals)
            down = lax.broadcasted_iota(jnp.int32, (pos_count, proposals), 0) + offset
            picked = down == lax.broadcasted_iota(jnp.int32, (pos_count, proposals), 1)
            across = lax.broadcasted_iota(jnp.int32, (proposals, pos_count), 1) + offset
            chosen = across == lax.broadcasted_iota(jnp.int32, (proposals, pos_count), 0)
            chosen = chosen.astype(F32).astype(BF16)
            along = lax.broadcasted_iota(jnp.int32, (1, pos_count), 1) + offset
            inside = (along >= 0) & (along < proposals)
            beneath = lax.broadcasted_iota(jnp.int32, (pos_count, 1), 0) + offset
            placed = jnp.dot(
                picked.astype(F32).astype(BF16),
                lat_rows[rows, qrank : qrank + kvrank],
                preferred_element_type=F32,
            )
            lat_out[j] = jnp.where(
                (beneath >= 0) & (beneath < proposals), placed, cache_lat[j].astype(F32)
            ).astype(BF16)
            new_rope = lat_rows[rows, qrank + kvrank :].astype(F32)[:, :rope_dim]
            swapped = jnp.concatenate([new_rope[:, half_dim:], new_rope[:, :half_dim]], axis=1)
            turned = (
                new_rope * query_cos[rows, :rope_dim] + swapped * query_sin[rows, :rope_dim]
            )
            contract = (((0,), (0,)), ((), ()))
            put = lax.dot_general(
                new_rope.astype(BF16), chosen, contract, preferred_element_type=F32
            )
            rope_out[j] = jnp.where(inside, put, rope32).astype(BF16)
            put = lax.dot_general(
                turned.astype(BF16), chosen, contract, preferred_element_type=F32
            )
            k_rot[j] = jnp.where(inside, put, k_rot[j].astype(F32)).astype(BF16)
            seen = jnp.dot(reach[s], chosen, preferred_element_type=F32)
            shown = jnp.where((seen > 0.5) | (along < 0), 0.0, HIDDEN)
            for h in range(heads):
                bias[j, h * proposals : (h + 1) * proposals, :] = shown

    for j in range(block):
        s = step * block + j
        keys = lat_out[j]
        score = lax.dot_general(
            q_lat[s], keys, (((1,), (1,)), ((), ())), preferred_element_type=F32
        )
        score = score + jnp.dot(
            q_rot[s][:, :rope_dim], k_rot[j], preferred_element_type=F32
        )
        score = score * scale + bias[j]
        top = jnp.maximum(jnp.max(score, axis=1, keepdims=True), LOWEST)
        weights = jnp.exp(score - top)
        total = jnp.sum(weights, axis=1, keepdims=True)
        numer[j] = jnp.dot(weights.astype(BF16), keys, preferred_element_type=F32)
        lane = lax.broadcasted_iota(jnp.int32, (1, 128), 1)
        terms = jnp.zeros((heads * proposals, 128), F32)
        for first, rest in ((0, top), (3, total)):
            for k in range(3):
                term = rest.astype(BF16).astype(F32)
                terms = jnp.where(lane == first + k, term, terms)
                rest = rest - term
        extra = jnp.transpose(terms)[:8].astype(BF16)
        for c in range(heads // 2):
            sent[j * (heads // 2) + c, 2 * proposals :, :] = extra

    for h in range(heads):
        part = numer[:, pl.ds(h * proposals, proposals), :].reshape(block * proposals, kvrank)
        upper = part.astype(BF16)
        lower = (part - upper.astype(F32)).astype(BF16)
        both = jnp.dot(
            jnp.concatenate([upper, lower], axis=0), w_value[h], preferred_element_type=F32
        )
        value = (both[: block * proposals] + both[block * proposals :]).astype(BF16)
        for j in range(block):
            sent[
                j * (heads // 2) + h // 2,
                (h % 2) * proposals : (h % 2 + 1) * proposals,
                :,
            ] = value[j * proposals : (j + 1) * proposals]


def attend(starts, base, lat_rows, weights, tables, reach, cache_lat, cache_rope):
    w_query, gain, w_key, w_value = weights
    seq_count, pos_count, kvrank = cache_lat.shape
    rope_dim = cache_rope.shape[1]
    heads, lanes, _ = w_key.shape
    proposals = reach.shape[2]
    rows = heads * proposals
    lat_width = w_query.shape[0] + kvrank + 128
    block = 4
    whole = pl.BlockSpec(memory_space=pltpu.VMEM)
    smem = pl.BlockSpec(memory_space=pltpu.SMEM)
    lat_spec = pl.BlockSpec((block, pos_count, kvrank), lambda g: (g, 0, 0))
    rope_spec = pl.BlockSpec((block, rope_dim, pos_count), lambda g: (g, 0, 0))
    chunks = heads // 2
    sent_shape = (seq_count * chunks, 2 * proposals + 8, w_value.shape[2])
    return pl.pallas_call(
        attend_kernel,
        grid=(seq_count // block,),
        in_specs=[smem, smem, *[whole] * 10, lat_spec, rope_spec],
        out_specs=[
            lat_spec,
            rope_spec,
            pl.BlockSpec((block * chunks, *sent_shape[1:]), lambda g: (g, 0, 0)),
        ],
        out_shape=[
            jax.ShapeDtypeStruct(cache_lat.shape, BF16),
            jax.ShapeDtypeStruct(cache_rope.shape, BF16),
            jax.ShapeDtypeStruct(sent_shape, BF16),
        ],
        scratch_shapes=[
            pltpu.VMEM((seq_count, rows, kvrank), BF16),
            pltpu.VMEM((seq_count, rows, lanes), BF16),
            pltpu.VMEM((block, rope_dim, pos_count), BF16),
            pltpu.VMEM((block, rows, pos_count), F32),
            pltpu.VMEM((block, rows, kvrank), F32),
            pltpu.VMEM((seq_count * proposals, lat_width), BF16),
        ],
        cost_estimate=pl.CostEstimate(
            flops=10**9, bytes_accessed=8 * 10**6, transcendentals=10**6
        ),
    )(starts, base, lat_rows, w_query, gain, w_key, w_value, *tables, reach, cache_lat, cache_rope)


def project_kernel(heads_in, w_out, result):
    seq_count, heads, proposals, vhead = heads_in.shape
    total = jnp.zeros(result.shape, F32)
    for h in range(heads):
        total += jnp.dot(
            heads_in[:, h].reshape(seq_count * proposals, vhead),
            w_out[:, h * vhead : (h + 1) * vhead].T,
            preferred_element_type=F32,
        )
    result[...] = total


def project(heads_in, w_out):
    seq_count, heads, proposals, vhead = heads_in.shape
    return pl.pallas_call(
        project_kernel,
        out_shape=jax.ShapeDtypeStruct((seq_count * proposals, w_out.shape[0]), F32),
        in_specs=[pl.BlockSpec(memory_space=pltpu.VMEM)] * 2,
        out_specs=pl.BlockSpec(memory_space=pltpu.VMEM),
        compiler_params=pltpu.CompilerParams(vmem_limit_bytes=8 * 1024 * 1024),
        cost_estimate=pl.CostEstimate(
            flops=2 * 10**7, bytes_accessed=6 * 10**5, transcendentals=0
        ),
    )(heads_in, w_out)


def local(
    tokens,
    gain_in,
    w_qdown,
    w_kvdown,
    w_ropek,
    gain_qlat,
    gain_kvlat,
    w_qup,
    gain_q,
    w_ukey,
    w_uval,
    w_out,
    gain_out,
    cache_lat,
    cache_rope,
    parents,
    lengths,
    accepted,
):
    seq_count, proposals, local_width = tokens.shape
    rows = seq_count * proposals
    owners = lax.axis_size(KV)
    full_width = local_width * lax.axis_size(KV_TP)
    qrank, heads_here, qkhead = w_qup.shape
    kvrank, _, nope_dim = w_ukey.shape
    vhead = w_uval.shape[2]
    rope_dim = cache_rope.shape[1]
    half_dim = rope_dim // 2

    half = rows // lax.axis_size("tp")
    inputs = gather_inputs(
        lax.axis_index(KV_TP)[None], tokens, gain_in, w_qdown, w_kvdown, w_ropek
    )
    inputs = lax.all_gather(inputs, "tp", axis=0, tiled=True)
    own_rows = lax.dynamic_slice_in_dim(inputs, lax.axis_index("tp") * half, half, 1)
    partial_rows = lax.dot_general(
        own_rows, inputs[:, rows:], (((0,), (0,)), ((), ())), preferred_element_type=F32
    )
    arrived = exchange(partial_rows.reshape(owners, half // owners, -1), KV)
    everyone = exchange(latents(arrived, full_width, gain_qlat, gain_kvlat), KV)
    everyone = lax.all_gather(everyone, "tp", axis=0, tiled=True)
    reaches, depths = ancestry(parents)
    starts = lengths + accepted
    angles = rope_angles(starts[:, None] + depths, half_dim).reshape(rows, half_dim)
    cosine, sine = jnp.cos(angles), jnp.sin(angles)
    lanes = qkhead + rope_dim
    spare = ((0, 0), (0, lanes - rope_dim))
    pos_count = cache_lat.shape[1]
    base = lax.axis_index(KV) * pos_count
    slot_angles = rope_angles(base + jnp.arange(pos_count, dtype=jnp.int32), half_dim).T
    tables = (
        jnp.pad(jnp.concatenate([cosine, cosine], axis=1), spare),
        jnp.pad(jnp.concatenate([-sine, sine], axis=1), spare),
        jnp.cos(slot_angles),
        jnp.sin(slot_angles),
    )

    def arranged(values):
        nope, low, high = jnp.split(values, [nope_dim, nope_dim + half_dim], axis=-1)
        return jnp.concatenate([low, high, nope, high, low], axis=-1)

    weights = (
        arranged(w_qup).reshape(qrank, heads_here * lanes),
        arranged(gain_q)[None],
        jnp.pad(jnp.transpose(w_ukey, (1, 2, 0)), ((0, 0), (rope_dim, rope_dim), (0, 0))),
        jnp.transpose(w_uval, (1, 0, 2)),
    )
    reach = reaches.astype(BF16)
    lat_out, rope_out, sent = attend(
        starts, base[None], everyone, weights, tables, reach, cache_lat, cache_rope
    )
    arrived = exchange(sent, KV).astype(F32)
    group = 2 * proposals
    chunk = lax.rem(lax.axis_index(KV), heads_here // 2)
    extras = lax.dynamic_slice_in_dim(arrived[:, group:], chunk * group, group, 2)
    maxima = extras[:, 0] + extras[:, 1] + extras[:, 2]
    denominators = extras[:, 3] + extras[:, 4] + extras[:, 5]
    factor = jnp.exp(maxima - jnp.max(maxima, axis=0))
    denom_all = jnp.sum(factor * denominators, axis=0)
    values_all = jnp.sum(factor[..., None] * arrived[:, :group], axis=0)
    head_share = (values_all / denom_all[:, None]).astype(BF16)
    head_rows = from_everyone(head_share, KV)
    partial_out = project(head_rows.reshape(seq_count, heads_here, proposals, vhead), w_out.T)
    mixed = lax.all_gather(partial_out, "tp").sum(axis=0)
    local_squares = jnp.sum(mixed * mixed, axis=-1)
    norm_total = from_everyone(local_squares[None], KV).sum(axis=(0, 1))
    own = lax.dynamic_slice_in_dim(mixed, lax.axis_index("tp") * local_width, local_width, 1)
    result = own * lax.rsqrt(norm_total / full_width + epsilon)[:, None] * gain_out
    result = result.astype(BF16).reshape(seq_count, proposals, local_width)
    return (result, lat_out, rope_out)


def solution(mesh):
    torus = Mesh(
        mesh.devices.reshape(mesh.shape["dp"], 8, 8, mesh.shape["tp"]), ("dp", "kv_0", "kv_1", "tp")
    )
    return jax.shard_map(
        local,
        mesh=torus,
        in_specs=(
            P("dp", None, KV_TP),
            P(KV_TP),
            P(KV_TP, None),
            P(KV_TP, None),
            P(),
            P(),
            P(),
            P(None, "tp", None),
            P(),
            P(None, "tp", None),
            P(None, "tp", None),
            P("tp", KV),
            P(KV_TP),
            P("dp", KV, None),
            P("dp", None, KV),
            P("dp", None),
            P("dp"),
            P("dp"),
        ),
        out_specs=(P("dp", None, KV_TP), P("dp", KV, None), P("dp", None, KV)),
        check_vma=False,
    )
```

```python
import functools

import jax
import jax.numpy as jnp
from jax import lax
from jax.experimental import pallas as pl
from jax.experimental.pallas import tpu as pltpu
from jax.sharding import Mesh
from jax.sharding import PartitionSpec as P

KV_TP = ("kv_0", "kv_1", "tp")
KV = ("kv_0", "kv_1")

epsilon = 1e-06
F32 = jnp.float32
BF16 = jnp.bfloat16
LOWEST = -1e30
HIDDEN = -3e38


def exchange(parts, axes):
    return lax.all_to_all(parts, axes, split_axis=0, concat_axis=0, tiled=True)


def from_everyone(shard, axes):
    return exchange(jnp.broadcast_to(shard[None], (lax.axis_size(axes), *shard.shape)), axes)


def normed(values, gain_vec):
    return (
        values * lax.rsqrt(jnp.mean(values * values, axis=-1, keepdims=True) + epsilon) * gain_vec
    )


def rope_angles(position, half_dim):
    frequency = 10000.0 ** (-(jnp.arange(half_dim, dtype=jnp.float32) * 2.0) / (2 * half_dim))
    return position.astype(jnp.float32)[..., None] * frequency


def ancestry(parents):
    proposals = parents.shape[-1]
    step = (parents[..., :, None] == jnp.arange(proposals, dtype=jnp.int32)).astype(BF16)
    reaches = step + jnp.eye(proposals, dtype=BF16)
    covered = 2
    while covered < proposals:
        step = jnp.einsum("sij,sjk->sik", step, step, preferred_element_type=F32).astype(BF16)
        reaches = reaches + jnp.einsum(
            "sij,sjk->sik", reaches, step, preferred_element_type=F32
        ).astype(BF16)
        covered *= 2
    reaches = reaches.astype(F32)
    depths = (jnp.sum(reaches, axis=-1) - 1.0).astype(jnp.int32)
    return (reaches, depths)


def gather_kernel(index, tokens, gain, w_qdown, w_kvdown, rope_columns, out):
    width = tokens.shape[2]
    rows = tokens.shape[0] * tokens.shape[1]
    qrank, kvrank = w_qdown.shape[1], w_kvdown.shape[1]
    rope_dim, lanes = rope_columns.shape
    tok_rows = tokens[...].astype(F32).reshape(rows, width)
    scaled = (tok_rows * gain[...]).astype(BF16).astype(F32)
    out[:width, :rows] = jnp.transpose(scaled).astype(BF16)
    out[:width, rows : rows + qrank] = w_qdown[...]
    out[:width, rows + qrank : rows + qrank + kvrank] = w_kvdown[...]
    at = rows + qrank + kvrank
    shift = lax.rem(lanes - lax.rem(index[0] * width, lanes), lanes)
    turned = pltpu.roll(rope_columns[...].astype(F32), shift, 1)
    padded = jnp.concatenate([turned, jnp.zeros((lanes - rope_dim, lanes), F32)], axis=0)
    out[:width, at:] = jnp.transpose(padded)[:width].astype(BF16)
    flipped = jnp.transpose(tok_rows)
    squares = jnp.sum(flipped * flipped, axis=0, keepdims=True)
    row = lax.broadcasted_iota(jnp.int32, (width, rows), 0)
    terms = jnp.zeros((width, rows), F32)
    for k in range(3):
        term = squares.astype(BF16).astype(F32)
        terms = jnp.where(row == k, term, terms)
        squares = squares - term
    out[width:, :rows] = terms.astype(BF16)
    out[width:, rows:at] = jnp.zeros((width, at - rows), BF16)
    row = lax.broadcasted_iota(jnp.int32, (width, lanes), 0)
    lane = lax.broadcasted_iota(jnp.int32, (width, lanes), 1)
    out[width:, at:] = jnp.where((row < 3) & (lane == rope_dim), 1.0, 0.0).astype(BF16)


def gather_inputs(index, tokens, gain_in, w_qdown, w_kvdown, w_ropek):
    width = tokens.shape[2]
    rows = tokens.shape[0] * tokens.shape[1]
    lanes = 128
    whole = pl.BlockSpec(memory_space=pltpu.VMEM)
    shape = (2 * width, rows + w_qdown.shape[1] + w_kvdown.shape[1] + lanes)
    return pl.pallas_call(
        gather_kernel,
        grid_spec=pltpu.PrefetchScalarGridSpec(
            num_scalar_prefetch=1,
            grid=(1,),
            in_specs=[
                *[whole] * 4,
                pl.BlockSpec(
                    (w_ropek.shape[1], lanes), lambda g, index: (0, index[0] * width // lanes)
                ),
            ],
            out_specs=whole,
        ),
        out_shape=jax.ShapeDtypeStruct(shape, BF16),
        cost_estimate=pl.CostEstimate(flops=10**5, bytes_accessed=10**5, transcendentals=0),
    )(index, tokens, gain_in[None], w_qdown, w_kvdown, w_ropek.T)


def latent_kernel(full_width, arrived, gain_qlat, gain_kvlat, out):
    qrank, kvrank = gain_qlat.shape[1], gain_kvlat.shape[1]
    summed = jnp.sum(arrived[...], axis=0)
    lanes = 128
    at = qrank + kvrank
    lane = lax.broadcasted_iota(jnp.int32, (1, lanes), 1)
    last = summed[:, at:]
    rope_dim = 32
    squares = jnp.sum(jnp.where(lane == rope_dim, last, 0.0), axis=1, keepdims=True)
    rescale = lax.rsqrt(squares / full_width + epsilon)
    share = jnp.concatenate(
        [
            normed(summed[:, :qrank] * rescale, gain_qlat[...]),
            normed(summed[:, qrank:at] * rescale, gain_kvlat[...]),
            jnp.where(lane < rope_dim, last * rescale, 0.0),
            jnp.zeros(last.shape, F32),
        ],
        axis=1,
    )
    pieces = [share[:, c * lanes : (c + 1) * lanes] for c in range(share.shape[1] // lanes)]
    stacked = jnp.concatenate(pieces, axis=0).astype(BF16)
    out[...] = jnp.broadcast_to(stacked[None], out.shape)


def latents(arrived, full_width, gain_qlat, gain_kvlat):
    owners = arrived.shape[0]
    return pl.pallas_call(
        functools.partial(latent_kernel, full_width),
        in_specs=[pl.BlockSpec(memory_space=pltpu.VMEM)] * 3,
        out_specs=pl.BlockSpec(memory_space=pltpu.VMEM),
        out_shape=jax.ShapeDtypeStruct((owners, 16, 128), BF16),
        compiler_params=pltpu.CompilerParams(vmem_limit_bytes=8 * 1024 * 1024),
        cost_estimate=pl.CostEstimate(flops=10**5, bytes_accessed=10**6, transcendentals=0),
    )(arrived, gain_qlat[None], gain_kvlat[None])


def attend_kernel(
    starts,
    base,
    packed,
    gain,
    query_turn,
    reach,
    w_query,
    w_key,
    w_value,
    key_turn,
    cache_rope,
    cache_lat,
    lat_out,
    rope_out,
    sent_out,
    q_lat,
    q_rot,
    k_rot,
    bias,
    numer,
    lat_rows,
    lat,
    rope,
    sent,
    lat_came,
    rope_came,
    lat_left,
    rope_left,
    sent_left,
):
    block = k_rot.shape[0]
    seq_count, pos_count, kvrank = cache_lat.shape
    qrank = w_query.shape[0]
    heads, lanes, _ = w_key.shape
    rope_dim = cache_rope.shape[1]
    half_dim = rope_dim // 2
    proposals = reach.shape[2]
    qkhead = lanes - rope_dim
    chunks = heads // 2
    scale = qkhead ** (-0.5)
    contract_last = (((1,), (1,)), ((), ()))
    contract_first = (((0,), (0,)), ((), ()))

    def coming(g):
        part = pl.ds(g * block, block)
        return (
            pltpu.make_async_copy(cache_lat.at[part], lat.at[part], lat_came.at[g]),
            pltpu.make_async_copy(cache_rope.at[part], rope.at[part], rope_came.at[g]),
        )

    def leaving(g):
        part = pl.ds(g * block, block)
        piece = pl.ds(g * block * chunks, block * chunks)
        return (
            pltpu.make_async_copy(lat.at[part], lat_out.at[part], lat_left.at[g]),
            pltpu.make_async_copy(rope.at[part], rope_out.at[part], rope_left.at[g]),
            pltpu.make_async_copy(sent.at[piece], sent_out.at[piece], sent_left.at[g]),
        )

    for g in range(seq_count // block):
        for copy in coming(g):
            copy.start()
    for c in range(lat_rows.shape[1] // 128):
        piece = packed[:, 2 * c : 2 * c + 2, :]
        lat_rows[:, c * 128 : (c + 1) * 128] = piece.reshape(lat_rows.shape[0], 128)
    lane = lax.broadcasted_iota(jnp.int32, (1, lanes), 1)
    cosine = jnp.where(lane < rope_dim, query_turn[...], 0.0)
    sine = jnp.where(lane < rope_dim, pltpu.roll(query_turn[...], lanes - rope_dim, 1), 0.0)
    projected = jnp.dot(lat_rows[:, :qrank], w_query[...], preferred_element_type=F32)
    for h in range(heads):
        one = projected[:, h * lanes : (h + 1) * lanes]
        mean = jnp.sum(jnp.where(lane < qkhead, one * one, 0.0), axis=1, keepdims=True) / qkhead
        one = one * lax.rsqrt(mean + epsilon) * gain[...]
        at = pl.ds(h * proposals, proposals)
        moved = jnp.dot(one.astype(BF16), w_key[h], preferred_element_type=F32)
        q_lat[:, at, :] = moved.astype(BF16).reshape(seq_count, proposals, kvrank)
        turned = one * cosine + pltpu.roll(one, rope_dim, 1) * sine
        q_rot[:, at, :] = turned.astype(BF16).reshape(seq_count, proposals, lanes)

    @pl.loop(0, seq_count // block)
    def _(step):
        for copy in coming(step):
            copy.wait()
        for j in range(block):
            s = step * block + j
            rope32 = rope[s].astype(F32)
            low, high = rope32[:half_dim], rope32[half_dim:]
            key_cos, key_sin = key_turn[:half_dim], key_turn[half_dim:]
            k_rot[j, :half_dim] = (low * key_cos - high * key_sin).astype(BF16)
            k_rot[j, half_dim:] = (high * key_cos + low * key_sin).astype(BF16)
            offset = base[0] - starts[s]
            hit = (offset > -pos_count) & (offset < proposals)

            @pl.when(jnp.logical_not(hit))
            def _():
                bias[j] = jnp.full(bias.shape[1:], jnp.where(offset < 0, 0.0, HIDDEN), F32)

            @pl.when(hit)
            def _():
                rows = pl.ds(pl.multiple_of(s * proposals, proposals), proposals)
                down = lax.broadcasted_iota(jnp.int32, (pos_count, proposals), 0) + offset
                picked = down == lax.broadcasted_iota(jnp.int32, (pos_count, proposals), 1)
                across = lax.broadcasted_iota(jnp.int32, (proposals, pos_count), 1) + offset
                chosen = across == lax.broadcasted_iota(jnp.int32, (proposals, pos_count), 0)
                chosen = chosen.astype(F32).astype(BF16)
                along = lax.broadcasted_iota(jnp.int32, (1, pos_count), 1) + offset
                inside = (along >= 0) & (along < proposals)
                beneath = lax.broadcasted_iota(jnp.int32, (pos_count, 1), 0) + offset
                placed = jnp.dot(
                    picked.astype(F32).astype(BF16),
                    lat_rows[rows, qrank : qrank + kvrank],
                    preferred_element_type=F32,
                )
                lat[s] = jnp.where(
                    (beneath >= 0) & (beneath < proposals), placed, lat[s].astype(F32)
                ).astype(BF16)
                new_rope = lat_rows[rows, qrank + kvrank :].astype(F32)[:, :rope_dim]
                swapped = jnp.concatenate(
                    [new_rope[:, half_dim:], new_rope[:, :half_dim]], axis=1
                )
                turn = query_turn[rows, :]
                turned = (
                    new_rope * turn[:, :rope_dim] + swapped * turn[:, rope_dim : 2 * rope_dim]
                )
                put = lax.dot_general(
                    new_rope.astype(BF16), chosen, contract_first, preferred_element_type=F32
                )
                rope[s] = jnp.where(inside, put, rope32).astype(BF16)
                put = lax.dot_general(
                    turned.astype(BF16), chosen, contract_first, preferred_element_type=F32
                )
                k_rot[j] = jnp.where(inside, put, k_rot[j].astype(F32)).astype(BF16)
                seen = jnp.dot(reach[s], chosen, preferred_element_type=F32)
                shown = jnp.where((seen > 0.5) | (along < 0), 0.0, HIDDEN)
                for h in range(heads):
                    bias[j, h * proposals : (h + 1) * proposals, :] = shown

        for j in range(block):
            s = step * block + j
            keys = lat[s]
            score = lax.dot_general(
                q_lat[s], keys, contract_last, preferred_element_type=F32
            )
            score = score + jnp.dot(
                q_rot[s][:, :rope_dim], k_rot[j], preferred_element_type=F32
            )
            score = score * scale + bias[j]
            top = jnp.maximum(jnp.max(score, axis=1, keepdims=True), LOWEST)
            weights = jnp.exp(score - top)
            total = jnp.sum(weights, axis=1, keepdims=True)
            numer[j] = jnp.dot(weights.astype(BF16), keys, preferred_element_type=F32)
            column = lax.broadcasted_iota(jnp.int32, (1, 128), 1)
            terms = jnp.zeros((heads * proposals, 128), F32)
            for first, rest in ((0, top), (3, total)):
                for k in range(3):
                    term = rest.astype(BF16).astype(F32)
                    terms = jnp.where(column == first + k, term, terms)
                    rest = rest - term
            extra = jnp.transpose(terms)[:8].astype(BF16)
            for c in range(chunks):
                sent[s * chunks + c, 2 * proposals :, :] = extra

        for h in range(heads):
            part = numer[:, pl.ds(h * proposals, proposals), :]
            part = part.reshape(block * proposals, kvrank)
            upper = part.astype(BF16)
            lower = (part - upper.astype(F32)).astype(BF16)
            both = jnp.dot(
                jnp.concatenate([upper, lower], axis=0), w_value[h], preferred_element_type=F32
            )
            value = (both[: block * proposals] + both[block * proposals :]).astype(BF16)
            for j in range(block):
                sent[
                    (step * block + j) * chunks + h // 2,
                    (h % 2) * proposals : (h % 2 + 1) * proposals,
                    :,
                ] = value[j * proposals : (j + 1) * proposals]
        for copy in leaving(step):
            copy.start()

    for g in range(seq_count // block):
        for copy in leaving(g):
            copy.wait()


def attend(starts, base, packed, gain, query_turn, reach, weights, key_turn, cache_rope, cache_lat):
    w_query, w_key, w_value = weights
    seq_count, pos_count, kvrank = cache_lat.shape
    rope_dim = cache_rope.shape[1]
    heads, lanes, _ = w_key.shape
    qrank = w_query.shape[0]
    proposals = reach.shape[2]
    rows = heads * proposals
    block = 4
    whole = pl.BlockSpec(memory_space=pltpu.VMEM)
    smem = pl.BlockSpec(memory_space=pltpu.SMEM)
    outside = pl.BlockSpec(memory_space=pltpu.HBM)
    sent_shape = (seq_count * heads // 2, 2 * proposals + 8, w_value.shape[2])
    groups = seq_count // block
    return pl.pallas_call(
        attend_kernel,
        in_specs=[smem, smem, *[whole] * 8, outside, outside],
        out_specs=[outside] * 3,
        out_shape=[
            pltpu.HBM(cache_lat.shape, BF16),
            pltpu.HBM(cache_rope.shape, BF16),
            pltpu.HBM(sent_shape, BF16),
        ],
        scratch_shapes=[
            pltpu.VMEM((seq_count, rows, kvrank), BF16),
            pltpu.VMEM((seq_count, rows, lanes), BF16),
            pltpu.VMEM((block, rope_dim, pos_count), BF16),
            pltpu.VMEM((block, rows, pos_count), F32),
            pltpu.VMEM((block, rows, kvrank), F32),
            pltpu.VMEM((seq_count * proposals, qrank + kvrank + 128), BF16),
            pltpu.VMEM(cache_lat.shape, BF16),
            pltpu.VMEM(cache_rope.shape, BF16),
            pltpu.VMEM(sent_shape, BF16),
            *[pltpu.SemaphoreType.DMA((groups,))] * 5,
        ],
        compiler_params=pltpu.CompilerParams(vmem_limit_bytes=50 * 1024 * 1024),
        cost_estimate=pl.CostEstimate(
            flops=10**9, bytes_accessed=8 * 10**6, transcendentals=10**6
        ),
    )(starts, base, packed, gain, query_turn, reach, *weights, key_turn, cache_rope, cache_lat)


def project_kernel(heads_in, w_out, result):
    seq_count, heads, proposals, vhead = heads_in.shape
    total = jnp.zeros(result.shape, F32)
    for h in range(heads):
        total += jnp.dot(
            heads_in[:, h].reshape(seq_count * proposals, vhead),
            w_out[:, h * vhead : (h + 1) * vhead].T,
            preferred_element_type=F32,
        )
    result[...] = total


def project(heads_in, w_out):
    seq_count, heads, proposals, vhead = heads_in.shape
    return pl.pallas_call(
        project_kernel,
        out_shape=jax.ShapeDtypeStruct((seq_count * proposals, w_out.shape[0]), F32),
        in_specs=[pl.BlockSpec(memory_space=pltpu.VMEM)] * 2,
        out_specs=pl.BlockSpec(memory_space=pltpu.VMEM),
        compiler_params=pltpu.CompilerParams(vmem_limit_bytes=8 * 1024 * 1024),
        cost_estimate=pl.CostEstimate(
            flops=2 * 10**7, bytes_accessed=6 * 10**5, transcendentals=0
        ),
    )(heads_in, w_out)


def local(
    tokens,
    gain_in,
    w_qdown,
    w_kvdown,
    w_ropek,
    gain_qlat,
    gain_kvlat,
    w_qup,
    gain_q,
    w_ukey,
    w_uval,
    w_out,
    gain_out,
    cache_lat,
    cache_rope,
    parents,
    lengths,
    accepted,
):
    seq_count, proposals, local_width = tokens.shape
    rows = seq_count * proposals
    owners = lax.axis_size(KV)
    full_width = local_width * lax.axis_size(KV_TP)
    qrank, heads_here, qkhead = w_qup.shape
    kvrank, _, nope_dim = w_ukey.shape
    vhead = w_uval.shape[2]
    rope_dim = cache_rope.shape[1]
    half_dim = rope_dim // 2

    half = rows // lax.axis_size("tp")
    inputs = gather_inputs(
        lax.axis_index(KV_TP)[None], tokens, gain_in, w_qdown, w_kvdown, w_ropek
    )
    inputs = lax.all_gather(inputs, "tp", axis=0, tiled=True)
    own_rows = lax.dynamic_slice_in_dim(inputs, lax.axis_index("tp") * half, half, 1)
    partial_rows = lax.dot_general(
        own_rows, inputs[:, rows:], (((0,), (0,)), ((), ())), preferred_element_type=F32
    )
    arrived = exchange(partial_rows.reshape(owners, half // owners, -1), KV)
    everyone = exchange(latents(arrived, full_width, gain_qlat, gain_kvlat), KV)
    everyone = lax.all_gather(everyone, "tp", axis=0, tiled=True)
    reaches, depths = ancestry(parents)
    starts = lengths + accepted
    angles = rope_angles(starts[:, None] + depths, half_dim).reshape(rows, half_dim)
    cosine, sine = jnp.cos(angles), jnp.sin(angles)
    lanes = qkhead + rope_dim
    pos_count = cache_lat.shape[1]
    base = lax.axis_index(KV) * pos_count
    slot_angles = rope_angles(base + jnp.arange(pos_count, dtype=jnp.int32), half_dim).T
    query_turn = jnp.pad(
        jnp.concatenate([cosine, cosine, -sine, sine], axis=1),
        ((0, 0), (0, lanes - 2 * rope_dim)),
    )
    key_turn = jnp.concatenate([jnp.cos(slot_angles), jnp.sin(slot_angles)], axis=0)

    def arranged(values):
        nope, low, high = jnp.split(values, [nope_dim, nope_dim + half_dim], axis=-1)
        return jnp.concatenate([low, high, nope, high, low], axis=-1)

    weights = (
        arranged(w_qup).reshape(qrank, heads_here * lanes),
        jnp.pad(jnp.transpose(w_ukey, (1, 2, 0)), ((0, 0), (rope_dim, rope_dim), (0, 0))),
        jnp.transpose(w_uval, (1, 0, 2)),
    )
    lat_out, rope_out, sent = attend(
        starts,
        base[None],
        everyone,
        arranged(gain_q)[None],
        query_turn,
        reaches.astype(BF16),
        weights,
        key_turn,
        cache_rope,
        cache_lat,
    )
    arrived = exchange(sent, KV).astype(F32)
    group = 2 * proposals
    chunk = lax.rem(lax.axis_index(KV), heads_here // 2)
    extras = lax.dynamic_slice_in_dim(arrived[:, group:], chunk * group, group, 2)
    maxima = extras[:, 0] + extras[:, 1] + extras[:, 2]
    denominators = extras[:, 3] + extras[:, 4] + extras[:, 5]
    factor = jnp.exp(maxima - jnp.max(maxima, axis=0))
    denom_all = jnp.sum(factor * denominators, axis=0)
    values_all = jnp.sum(factor[..., None] * arrived[:, :group], axis=0)
    head_share = (values_all / denom_all[:, None]).astype(BF16)
    head_rows = from_everyone(head_share, KV)
    partial_out = project(head_rows.reshape(seq_count, heads_here, proposals, vhead), w_out.T)
    mixed = lax.all_gather(partial_out, "tp").sum(axis=0)
    local_squares = jnp.sum(mixed * mixed, axis=-1)
    norm_total = from_everyone(local_squares[None], KV).sum(axis=(0, 1))
    own = lax.dynamic_slice_in_dim(mixed, lax.axis_index("tp") * local_width, local_width, 1)
    result = own * lax.rsqrt(norm_total / full_width + epsilon)[:, None] * gain_out
    result = result.astype(BF16).reshape(seq_count, proposals, local_width)
    return (result, lat_out, rope_out)


def solution(mesh):
    torus = Mesh(
        mesh.devices.reshape(mesh.shape["dp"], 8, 8, mesh.shape["tp"]), ("dp", "kv_0", "kv_1", "tp")
    )
    return jax.shard_map(
        local,
        mesh=torus,
        in_specs=(
            P("dp", None, KV_TP),
            P(KV_TP),
            P(KV_TP, None),
            P(KV_TP, None),
            P(),
            P(),
            P(),
            P(None, "tp", None),
            P(),
            P(None, "tp", None),
            P(None, "tp", None),
            P("tp", KV),
            P(KV_TP),
            P("dp", KV, None),
            P("dp", None, KV),
            P("dp", None),
            P("dp"),
            P("dp"),
        ),
        out_specs=(P("dp", None, KV_TP), P("dp", KV, None), P("dp", None, KV)),
        check_vma=False,
    )
```

```python
import functools

import jax
import jax.numpy as jnp
from jax import lax
from jax.experimental import pallas as pl
from jax.experimental.pallas import tpu as pltpu
from jax.sharding import Mesh
from jax.sharding import PartitionSpec as P

KV_TP = ("kv_0", "kv_1", "tp")
KV = ("kv_0", "kv_1")

epsilon = 1e-06
F32 = jnp.float32
BF16 = jnp.bfloat16
LOWEST = -1e30
HIDDEN = -3e38


def exchange(parts, axes):
    return lax.all_to_all(parts, axes, split_axis=0, concat_axis=0, tiled=True)


def from_everyone(shard, axes):
    return exchange(jnp.broadcast_to(shard[None], (lax.axis_size(axes), *shard.shape)), axes)


def normed(values, gain_vec):
    return (
        values * lax.rsqrt(jnp.mean(values * values, axis=-1, keepdims=True) + epsilon) * gain_vec
    )


def rope_angles(position, half_dim):
    frequency = 10000.0 ** (-(jnp.arange(half_dim, dtype=jnp.float32) * 2.0) / (2 * half_dim))
    return position.astype(jnp.float32)[..., None] * frequency


def ancestry(parents):
    proposals = parents.shape[-1]
    step = (parents[..., :, None] == jnp.arange(proposals, dtype=jnp.int32)).astype(BF16)
    reaches = step + jnp.eye(proposals, dtype=BF16)
    covered = 2
    while covered < proposals:
        step = jnp.einsum("sij,sjk->sik", step, step, preferred_element_type=F32).astype(BF16)
        reaches = reaches + jnp.einsum(
            "sij,sjk->sik", reaches, step, preferred_element_type=F32
        ).astype(BF16)
        covered *= 2
    reaches = reaches.astype(F32)
    depths = (jnp.sum(reaches, axis=-1) - 1.0).astype(jnp.int32)
    return (reaches, depths)


def gather_kernel(index, tokens, gain, w_qdown, w_kvdown, rope_columns, out):
    width = tokens.shape[2]
    rows = tokens.shape[0] * tokens.shape[1]
    qrank, kvrank = w_qdown.shape[1], w_kvdown.shape[1]
    rope_dim, lanes = rope_columns.shape
    tok_rows = tokens[...].astype(F32).reshape(rows, width)
    scaled = (tok_rows * gain[...]).astype(BF16).astype(F32)
    out[:width, :rows] = jnp.transpose(scaled).astype(BF16)
    out[:width, rows : rows + qrank] = w_qdown[...]
    out[:width, rows + qrank : rows + qrank + kvrank] = w_kvdown[...]
    at = rows + qrank + kvrank
    shift = lax.rem(lanes - lax.rem(index[0] * width, lanes), lanes)
    turned = pltpu.roll(rope_columns[...].astype(F32), shift, 1)
    padded = jnp.concatenate([turned, jnp.zeros((lanes - rope_dim, lanes), F32)], axis=0)
    out[:width, at:] = jnp.transpose(padded)[:width].astype(BF16)
    flipped = jnp.transpose(tok_rows)
    squares = jnp.sum(flipped * flipped, axis=0, keepdims=True)
    row = lax.broadcasted_iota(jnp.int32, (width, rows), 0)
    terms = jnp.zeros((width, rows), F32)
    for k in range(3):
        term = squares.astype(BF16).astype(F32)
        terms = jnp.where(row == k, term, terms)
        squares = squares - term
    out[width:, :rows] = terms.astype(BF16)
    out[width:, rows:at] = jnp.zeros((width, at - rows), BF16)
    row = lax.broadcasted_iota(jnp.int32, (width, lanes), 0)
    lane = lax.broadcasted_iota(jnp.int32, (width, lanes), 1)
    out[width:, at:] = jnp.where((row < 3) & (lane == rope_dim), 1.0, 0.0).astype(BF16)


def gather_inputs(index, tokens, gain_in, w_qdown, w_kvdown, w_ropek):
    width = tokens.shape[2]
    rows = tokens.shape[0] * tokens.shape[1]
    lanes = 128
    whole = pl.BlockSpec(memory_space=pltpu.VMEM)
    shape = (2 * width, rows + w_qdown.shape[1] + w_kvdown.shape[1] + lanes)
    return pl.pallas_call(
        gather_kernel,
        grid_spec=pltpu.PrefetchScalarGridSpec(
            num_scalar_prefetch=1,
            grid=(1,),
            in_specs=[
                *[whole] * 4,
                pl.BlockSpec(
                    (w_ropek.shape[1], lanes), lambda g, index: (0, index[0] * width // lanes)
                ),
            ],
            out_specs=whole,
        ),
        out_shape=pltpu.VMEM(shape, BF16),
        cost_estimate=pl.CostEstimate(flops=10**5, bytes_accessed=10**5, transcendentals=0),
    )(index, tokens, gain_in[None], w_qdown, w_kvdown, w_ropek.T)


def latent_kernel(full_width, arrived, gain_qlat, gain_kvlat, out):
    qrank, kvrank = gain_qlat.shape[1], gain_kvlat.shape[1]
    summed = jnp.sum(arrived[...], axis=0)
    lanes = 128
    at = qrank + kvrank
    lane = lax.broadcasted_iota(jnp.int32, (1, lanes), 1)
    last = summed[:, at:]
    rope_dim = 32
    squares = jnp.sum(jnp.where(lane == rope_dim, last, 0.0), axis=1, keepdims=True)
    rescale = lax.rsqrt(squares / full_width + epsilon)
    share = jnp.concatenate(
        [
            normed(summed[:, :qrank] * rescale, gain_qlat[...]),
            normed(summed[:, qrank:at] * rescale, gain_kvlat[...]),
            jnp.where(lane < rope_dim, last * rescale, 0.0),
            jnp.zeros(last.shape, F32),
        ],
        axis=1,
    )
    pieces = [share[:, c * lanes : (c + 1) * lanes] for c in range(share.shape[1] // lanes)]
    stacked = jnp.concatenate(pieces, axis=0).astype(BF16)
    out[...] = jnp.broadcast_to(stacked[None], out.shape)


def latents(arrived, full_width, gain_qlat, gain_kvlat):
    owners = arrived.shape[0]
    return pl.pallas_call(
        functools.partial(latent_kernel, full_width),
        in_specs=[pl.BlockSpec(memory_space=pltpu.VMEM)] * 3,
        out_specs=pl.BlockSpec(memory_space=pltpu.VMEM),
        out_shape=jax.ShapeDtypeStruct((owners, 16, 128), BF16),
        compiler_params=pltpu.CompilerParams(vmem_limit_bytes=8 * 1024 * 1024),
        cost_estimate=pl.CostEstimate(flops=10**5, bytes_accessed=10**6, transcendentals=0),
    )(arrived, gain_qlat[None], gain_kvlat[None])


def attend_kernel(
    starts,
    base,
    packed,
    gain,
    query_turn,
    reach,
    w_query,
    w_key,
    w_value,
    key_turn,
    cache_rope,
    cache_lat,
    lat_out,
    rope_out,
    sent_out,
    q_lat,
    q_rot,
    k_rot,
    bias,
    numer,
    lat_rows,
    lat,
    rope,
    sent,
    lat_came,
    rope_came,
    lat_left,
    rope_left,
    sent_left,
):
    block = k_rot.shape[0]
    seq_count, pos_count, kvrank = cache_lat.shape
    qrank = w_query.shape[0]
    heads, lanes, _ = w_key.shape
    rope_dim = cache_rope.shape[1]
    half_dim = rope_dim // 2
    proposals = reach.shape[2]
    qkhead = lanes - rope_dim
    chunks = heads // 2
    scale = qkhead ** (-0.5)
    contract_last = (((1,), (1,)), ((), ()))
    contract_first = (((0,), (0,)), ((), ()))

    def coming(g):
        part = pl.ds(g * block, block)
        return (
            pltpu.make_async_copy(cache_lat.at[part], lat.at[part], lat_came.at[g]),
            pltpu.make_async_copy(cache_rope.at[part], rope.at[part], rope_came.at[g]),
        )

    def leaving(g):
        part = pl.ds(g * block, block)
        piece = pl.ds(g * block * chunks, block * chunks)
        return (
            pltpu.make_async_copy(lat.at[part], lat_out.at[part], lat_left.at[g]),
            pltpu.make_async_copy(rope.at[part], rope_out.at[part], rope_left.at[g]),
            pltpu.make_async_copy(sent.at[piece], sent_out.at[piece], sent_left.at[g]),
        )

    for g in range(seq_count // block):
        for copy in coming(g):
            copy.start()
    for c in range(lat_rows.shape[1] // 128):
        piece = packed[:, 2 * c : 2 * c + 2, :]
        lat_rows[:, c * 128 : (c + 1) * 128] = piece.reshape(lat_rows.shape[0], 128)
    lane = lax.broadcasted_iota(jnp.int32, (1, lanes), 1)
    cosine = jnp.where(lane < rope_dim, query_turn[...], 0.0)
    sine = jnp.where(lane < rope_dim, pltpu.roll(query_turn[...], lanes - rope_dim, 1), 0.0)
    projected = jnp.dot(lat_rows[:, :qrank], w_query[...], preferred_element_type=F32)
    for h in range(heads):
        one = projected[:, h * lanes : (h + 1) * lanes]
        mean = jnp.sum(jnp.where(lane < qkhead, one * one, 0.0), axis=1, keepdims=True) / qkhead
        one = one * lax.rsqrt(mean + epsilon) * gain[...]
        at = pl.ds(h * proposals, proposals)
        moved = jnp.dot(one.astype(BF16), w_key[h], preferred_element_type=F32)
        q_lat[:, at, :] = moved.astype(BF16).reshape(seq_count, proposals, kvrank)
        turned = one * cosine + pltpu.roll(one, rope_dim, 1) * sine
        q_rot[:, at, :] = turned.astype(BF16).reshape(seq_count, proposals, lanes)

    @pl.loop(0, seq_count // block)
    def _(step):
        for copy in coming(step):
            copy.wait()
        for j in range(block):
            s = step * block + j
            rope32 = rope[s].astype(F32)
            low, high = rope32[:half_dim], rope32[half_dim:]
            key_cos, key_sin = key_turn[:half_dim], key_turn[half_dim:]
            k_rot[j, :half_dim] = (low * key_cos - high * key_sin).astype(BF16)
            k_rot[j, half_dim:] = (high * key_cos + low * key_sin).astype(BF16)
            offset = base[0] - starts[s]
            hit = (offset > -pos_count) & (offset < proposals)

            @pl.when(jnp.logical_not(hit))
            def _():
                bias[j] = jnp.full(bias.shape[1:], jnp.where(offset < 0, 0.0, HIDDEN), F32)

            @pl.when(hit)
            def _():
                rows = pl.ds(pl.multiple_of(s * proposals, proposals), proposals)
                down = lax.broadcasted_iota(jnp.int32, (pos_count, proposals), 0) + offset
                picked = down == lax.broadcasted_iota(jnp.int32, (pos_count, proposals), 1)
                across = lax.broadcasted_iota(jnp.int32, (proposals, pos_count), 1) + offset
                chosen = across == lax.broadcasted_iota(jnp.int32, (proposals, pos_count), 0)
                chosen = chosen.astype(F32).astype(BF16)
                along = lax.broadcasted_iota(jnp.int32, (1, pos_count), 1) + offset
                inside = (along >= 0) & (along < proposals)
                beneath = lax.broadcasted_iota(jnp.int32, (pos_count, 1), 0) + offset
                placed = jnp.dot(
                    picked.astype(F32).astype(BF16),
                    lat_rows[rows, qrank : qrank + kvrank],
                    preferred_element_type=F32,
                )
                lat[s] = jnp.where(
                    (beneath >= 0) & (beneath < proposals), placed, lat[s].astype(F32)
                ).astype(BF16)
                new_rope = lat_rows[rows, qrank + kvrank :].astype(F32)[:, :rope_dim]
                swapped = jnp.concatenate(
                    [new_rope[:, half_dim:], new_rope[:, :half_dim]], axis=1
                )
                turn = query_turn[rows, :]
                turned = (
                    new_rope * turn[:, :rope_dim] + swapped * turn[:, rope_dim : 2 * rope_dim]
                )
                put = lax.dot_general(
                    new_rope.astype(BF16), chosen, contract_first, preferred_element_type=F32
                )
                rope[s] = jnp.where(inside, put, rope32).astype(BF16)
                put = lax.dot_general(
                    turned.astype(BF16), chosen, contract_first, preferred_element_type=F32
                )
                k_rot[j] = jnp.where(inside, put, k_rot[j].astype(F32)).astype(BF16)
                seen = jnp.dot(reach[s], chosen, preferred_element_type=F32)
                shown = jnp.where((seen > 0.5) | (along < 0), 0.0, HIDDEN)
                for h in range(heads):
                    bias[j, h * proposals : (h + 1) * proposals, :] = shown

        for copy in leaving(step)[:2]:
            copy.start()
        for j in range(block):
            s = step * block + j
            keys = lat[s]
            score = lax.dot_general(
                q_lat[s], keys, contract_last, preferred_element_type=F32
            )
            score = score + jnp.dot(
                q_rot[s][:, :rope_dim], k_rot[j], preferred_element_type=F32
            )
            score = score * scale + bias[j]
            top = jnp.maximum(jnp.max(score, axis=1, keepdims=True), LOWEST)
            weights = jnp.exp(score - top)
            total = jnp.sum(weights, axis=1, keepdims=True)
            numer[j] = jnp.dot(weights.astype(BF16), keys, preferred_element_type=F32)
            column = lax.broadcasted_iota(jnp.int32, (1, 128), 1)
            terms = jnp.zeros((heads * proposals, 128), F32)
            for first, rest in ((0, top), (3, total)):
                for k in range(3):
                    term = rest.astype(BF16).astype(F32)
                    terms = jnp.where(column == first + k, term, terms)
                    rest = rest - term
            extra = jnp.transpose(terms)[:8].astype(BF16)
            for c in range(chunks):
                sent[s * chunks + c, 2 * proposals :, :] = extra

        for h in range(heads):
            part = numer[:, pl.ds(h * proposals, proposals), :]
            part = part.reshape(block * proposals, kvrank)
            upper = part.astype(BF16)
            lower = (part - upper.astype(F32)).astype(BF16)
            both = jnp.dot(
                jnp.concatenate([upper, lower], axis=0), w_value[h], preferred_element_type=F32
            )
            value = (both[: block * proposals] + both[block * proposals :]).astype(BF16)
            for j in range(block):
                sent[
                    (step * block + j) * chunks + h // 2,
                    (h % 2) * proposals : (h % 2 + 1) * proposals,
                    :,
                ] = value[j * proposals : (j + 1) * proposals]
        leaving(step)[2].start()

    for g in range(seq_count // block):
        for copy in leaving(g):
            copy.wait()


def attend(starts, base, packed, gain, query_turn, reach, weights, key_turn, cache_rope, cache_lat):
    w_query, w_key, w_value = weights
    seq_count, pos_count, kvrank = cache_lat.shape
    rope_dim = cache_rope.shape[1]
    heads, lanes, _ = w_key.shape
    qrank = w_query.shape[0]
    proposals = reach.shape[2]
    rows = heads * proposals
    block = 16
    whole = pl.BlockSpec(memory_space=pltpu.VMEM)
    smem = pl.BlockSpec(memory_space=pltpu.SMEM)
    outside = pl.BlockSpec(memory_space=pltpu.HBM)
    sent_shape = (seq_count * heads // 2, 2 * proposals + 8, w_value.shape[2])
    groups = seq_count // block
    return pl.pallas_call(
        attend_kernel,
        in_specs=[smem, smem, *[whole] * 8, outside, outside],
        out_specs=[outside] * 3,
        out_shape=[
            pltpu.HBM(cache_lat.shape, BF16),
            pltpu.HBM(cache_rope.shape, BF16),
            pltpu.HBM(sent_shape, BF16),
        ],
        scratch_shapes=[
            pltpu.VMEM((seq_count, rows, kvrank), BF16),
            pltpu.VMEM((seq_count, rows, lanes), BF16),
            pltpu.VMEM((block, rope_dim, pos_count), BF16),
            pltpu.VMEM((block, rows, pos_count), F32),
            pltpu.VMEM((block, rows, kvrank), F32),
            pltpu.VMEM((seq_count * proposals, qrank + kvrank + 128), BF16),
            pltpu.VMEM(cache_lat.shape, BF16),
            pltpu.VMEM(cache_rope.shape, BF16),
            pltpu.VMEM(sent_shape, BF16),
            *[pltpu.SemaphoreType.DMA((groups,))] * 5,
        ],
        compiler_params=pltpu.CompilerParams(vmem_limit_bytes=50 * 1024 * 1024),
        cost_estimate=pl.CostEstimate(
            flops=10**9, bytes_accessed=8 * 10**6, transcendentals=10**6
        ),
    )(starts, base, packed, gain, query_turn, reach, *weights, key_turn, cache_rope, cache_lat)


def project_kernel(heads_in, w_out, result):
    seq_count, heads, proposals, vhead = heads_in.shape
    total = jnp.zeros(result.shape, F32)
    for h in range(heads):
        total += jnp.dot(
            heads_in[:, h].reshape(seq_count * proposals, vhead),
            w_out[:, h * vhead : (h + 1) * vhead].T,
            preferred_element_type=F32,
        )
    result[...] = total


def project(heads_in, w_out):
    seq_count, heads, proposals, vhead = heads_in.shape
    return pl.pallas_call(
        project_kernel,
        out_shape=jax.ShapeDtypeStruct((seq_count * proposals, w_out.shape[0]), F32),
        in_specs=[pl.BlockSpec(memory_space=pltpu.VMEM)] * 2,
        out_specs=pl.BlockSpec(memory_space=pltpu.VMEM),
        compiler_params=pltpu.CompilerParams(vmem_limit_bytes=8 * 1024 * 1024),
        cost_estimate=pl.CostEstimate(
            flops=2 * 10**7, bytes_accessed=6 * 10**5, transcendentals=0
        ),
    )(heads_in, w_out)


def local(
    tokens,
    gain_in,
    w_qdown,
    w_kvdown,
    w_ropek,
    gain_qlat,
    gain_kvlat,
    w_qup,
    gain_q,
    w_ukey,
    w_uval,
    w_out,
    gain_out,
    cache_lat,
    cache_rope,
    parents,
    lengths,
    accepted,
):
    seq_count, proposals, local_width = tokens.shape
    rows = seq_count * proposals
    owners = lax.axis_size(KV)
    full_width = local_width * lax.axis_size(KV_TP)
    qrank, heads_here, qkhead = w_qup.shape
    kvrank, _, nope_dim = w_ukey.shape
    vhead = w_uval.shape[2]
    rope_dim = cache_rope.shape[1]
    half_dim = rope_dim // 2

    half = rows // lax.axis_size("tp")
    inputs = gather_inputs(
        lax.axis_index(KV_TP)[None], tokens, gain_in, w_qdown, w_kvdown, w_ropek
    )
    inputs = lax.all_gather(inputs, "tp", axis=0, tiled=True)
    own_rows = lax.dynamic_slice_in_dim(inputs, lax.axis_index("tp") * half, half, 1)
    partial_rows = lax.dot_general(
        own_rows, inputs[:, rows:], (((0,), (0,)), ((), ())), preferred_element_type=F32
    )
    arrived = exchange(partial_rows.reshape(owners, half // owners, -1), KV)
    everyone = exchange(latents(arrived, full_width, gain_qlat, gain_kvlat), KV)
    everyone = lax.all_gather(everyone, "tp", axis=0, tiled=True)
    reaches, depths = ancestry(parents)
    starts = lengths + accepted
    angles = rope_angles(starts[:, None] + depths, half_dim).reshape(rows, half_dim)
    cosine, sine = jnp.cos(angles), jnp.sin(angles)
    lanes = qkhead + rope_dim
    pos_count = cache_lat.shape[1]
    base = lax.axis_index(KV) * pos_count
    slot_angles = rope_angles(base + jnp.arange(pos_count, dtype=jnp.int32), half_dim).T
    query_turn = jnp.pad(
        jnp.concatenate([cosine, cosine, -sine, sine], axis=1),
        ((0, 0), (0, lanes - 2 * rope_dim)),
    )
    key_turn = jnp.concatenate([jnp.cos(slot_angles), jnp.sin(slot_angles)], axis=0)

    def arranged(values):
        nope, low, high = jnp.split(values, [nope_dim, nope_dim + half_dim], axis=-1)
        return jnp.concatenate([low, high, nope, high, low], axis=-1)

    weights = (
        arranged(w_qup).reshape(qrank, heads_here * lanes),
        jnp.pad(jnp.transpose(w_ukey, (1, 2, 0)), ((0, 0), (rope_dim, rope_dim), (0, 0))),
        jnp.transpose(w_uval, (1, 0, 2)),
    )
    lat_out, rope_out, sent = attend(
        starts,
        base[None],
        everyone,
        arranged(gain_q)[None],
        query_turn,
        reaches.astype(BF16),
        weights,
        key_turn,
        cache_rope,
        cache_lat,
    )
    arrived = exchange(sent, KV).astype(F32)
    group = 2 * proposals
    chunk = lax.rem(lax.axis_index(KV), heads_here // 2)
    extras = lax.dynamic_slice_in_dim(arrived[:, group:], chunk * group, group, 2)
    maxima = extras[:, 0] + extras[:, 1] + extras[:, 2]
    denominators = extras[:, 3] + extras[:, 4] + extras[:, 5]
    factor = jnp.exp(maxima - jnp.max(maxima, axis=0))
    denom_all = jnp.sum(factor * denominators, axis=0)
    values_all = jnp.sum(factor[..., None] * arrived[:, :group], axis=0)
    head_share = (values_all / denom_all[:, None]).astype(BF16)
    head_rows = from_everyone(head_share, KV)
    partial_out = project(head_rows.reshape(seq_count, heads_here, proposals, vhead), w_out.T)
    mixed = lax.all_gather(partial_out, "tp").sum(axis=0)
    local_squares = jnp.sum(mixed * mixed, axis=-1)
    norm_total = from_everyone(local_squares[None], KV).sum(axis=(0, 1))
    own = lax.dynamic_slice_in_dim(mixed, lax.axis_index("tp") * local_width, local_width, 1)
    result = own * lax.rsqrt(norm_total / full_width + epsilon)[:, None] * gain_out
    result = result.astype(BF16).reshape(seq_count, proposals, local_width)
    return (result, lat_out, rope_out)


def solution(mesh):
    torus = Mesh(
        mesh.devices.reshape(mesh.shape["dp"], 8, 8, mesh.shape["tp"]), ("dp", "kv_0", "kv_1", "tp")
    )
    return jax.shard_map(
        local,
        mesh=torus,
        in_specs=(
            P("dp", None, KV_TP),
            P(KV_TP),
            P(KV_TP, None),
            P(KV_TP, None),
            P(),
            P(),
            P(),
            P(None, "tp", None),
            P(),
            P(None, "tp", None),
            P(None, "tp", None),
            P("tp", KV),
            P(KV_TP),
            P("dp", KV, None),
            P("dp", None, KV),
            P("dp", None),
            P("dp"),
            P("dp"),
        ),
        out_specs=(P("dp", None, KV_TP), P("dp", KV, None), P("dp", None, KV)),
        check_vma=False,
    )
```

```python
import functools

import jax
import jax.numpy as jnp
from jax import lax
from jax.experimental import pallas as pl
from jax.experimental.pallas import tpu as pltpu
from jax.sharding import Mesh
from jax.sharding import PartitionSpec as P

KV_TP = ("kv_0", "kv_1", "tp")
KV = ("kv_0", "kv_1")

epsilon = 1e-06
F32 = jnp.float32
BF16 = jnp.bfloat16
LOWEST = -1e30
HIDDEN = -3e38


def exchange(parts, axes):
    return lax.all_to_all(parts, axes, split_axis=0, concat_axis=0, tiled=True)


def from_everyone(shard, axes):
    return exchange(jnp.broadcast_to(shard[None], (lax.axis_size(axes), *shard.shape)), axes)


def normed(values, gain_vec):
    return (
        values * lax.rsqrt(jnp.mean(values * values, axis=-1, keepdims=True) + epsilon) * gain_vec
    )


def rope_angles(position, half_dim):
    frequency = 10000.0 ** (-(jnp.arange(half_dim, dtype=jnp.float32) * 2.0) / (2 * half_dim))
    return position.astype(jnp.float32)[..., None] * frequency


def ancestry(parents):
    proposals = parents.shape[-1]
    step = (parents[..., :, None] == jnp.arange(proposals, dtype=jnp.int32)).astype(BF16)
    reaches = step + jnp.eye(proposals, dtype=BF16)
    covered = 2
    while covered < proposals:
        step = jnp.einsum("sij,sjk->sik", step, step, preferred_element_type=F32).astype(BF16)
        reaches = reaches + jnp.einsum(
            "sij,sjk->sik", reaches, step, preferred_element_type=F32
        ).astype(BF16)
        covered *= 2
    reaches = reaches.astype(F32)
    depths = (jnp.sum(reaches, axis=-1) - 1.0).astype(jnp.int32)
    return (reaches, depths)


def gather_kernel(index, tokens, gain, w_qdown, w_kvdown, rope_columns, out):
    width = tokens.shape[2]
    rows = tokens.shape[0] * tokens.shape[1]
    qrank, kvrank = w_qdown.shape[1], w_kvdown.shape[1]
    rope_dim, lanes = rope_columns.shape
    tok_rows = tokens[...].astype(F32).reshape(rows, width)
    scaled = (tok_rows * gain[...]).astype(BF16).astype(F32)
    out[:width, :rows] = jnp.transpose(scaled).astype(BF16)
    out[:width, rows : rows + qrank] = w_qdown[...]
    out[:width, rows + qrank : rows + qrank + kvrank] = w_kvdown[...]
    at = rows + qrank + kvrank
    shift = lax.rem(lanes - lax.rem(index[0] * width, lanes), lanes)
    turned = pltpu.roll(rope_columns[...].astype(F32), shift, 1)
    padded = jnp.concatenate([turned, jnp.zeros((lanes - rope_dim, lanes), F32)], axis=0)
    out[:width, at:] = jnp.transpose(padded)[:width].astype(BF16)
    flipped = jnp.transpose(tok_rows)
    squares = jnp.sum(flipped * flipped, axis=0, keepdims=True)
    row = lax.broadcasted_iota(jnp.int32, (width, rows), 0)
    terms = jnp.zeros((width, rows), F32)
    for k in range(3):
        term = squares.astype(BF16).astype(F32)
        terms = jnp.where(row == k, term, terms)
        squares = squares - term
    out[width:, :rows] = terms.astype(BF16)
    out[width:, rows:at] = jnp.zeros((width, at - rows), BF16)
    row = lax.broadcasted_iota(jnp.int32, (width, lanes), 0)
    lane = lax.broadcasted_iota(jnp.int32, (width, lanes), 1)
    out[width:, at:] = jnp.where((row < 3) & (lane == rope_dim), 1.0, 0.0).astype(BF16)


def gather_inputs(index, tokens, gain_in, w_qdown, w_kvdown, w_ropek):
    width = tokens.shape[2]
    rows = tokens.shape[0] * tokens.shape[1]
    lanes = 128
    whole = pl.BlockSpec(memory_space=pltpu.VMEM)
    shape = (2 * width, rows + w_qdown.shape[1] + w_kvdown.shape[1] + lanes)
    return pl.pallas_call(
        gather_kernel,
        grid_spec=pltpu.PrefetchScalarGridSpec(
            num_scalar_prefetch=1,
            grid=(1,),
            in_specs=[
                *[whole] * 4,
                pl.BlockSpec(
                    (w_ropek.shape[1], lanes), lambda g, index: (0, index[0] * width // lanes)
                ),
            ],
            out_specs=whole,
        ),
        out_shape=pltpu.VMEM(shape, BF16),
        cost_estimate=pl.CostEstimate(flops=10**5, bytes_accessed=10**5, transcendentals=0),
    )(index, tokens, gain_in[None], w_qdown, w_kvdown, w_ropek.T)


def latent_kernel(full_width, arrived, gain_qlat, gain_kvlat, out):
    qrank, kvrank = gain_qlat.shape[1], gain_kvlat.shape[1]
    summed = jnp.sum(arrived[...], axis=0)
    lanes = 128
    at = qrank + kvrank
    lane = lax.broadcasted_iota(jnp.int32, (1, lanes), 1)
    last = summed[:, at:]
    rope_dim = 32
    squares = jnp.sum(jnp.where(lane == rope_dim, last, 0.0), axis=1, keepdims=True)
    rescale = lax.rsqrt(squares / full_width + epsilon)
    share = jnp.concatenate(
        [
            normed(summed[:, :qrank] * rescale, gain_qlat[...]),
            normed(summed[:, qrank:at] * rescale, gain_kvlat[...]),
            jnp.where(lane < rope_dim, last * rescale, 0.0),
        ],
        axis=1,
    )
    for c in range(share.shape[1] // lanes):
        piece = share[:, c * lanes : (c + 1) * lanes].astype(BF16)
        out[:, c] = jnp.broadcast_to(piece[None], (out.shape[0], *piece.shape))


def latents(arrived, full_width, gain_qlat, gain_kvlat):
    owners = arrived.shape[0]
    return pl.pallas_call(
        functools.partial(latent_kernel, full_width),
        in_specs=[pl.BlockSpec(memory_space=pltpu.VMEM)] * 3,
        out_specs=pl.BlockSpec(memory_space=pltpu.VMEM),
        out_shape=jax.ShapeDtypeStruct(
            (owners, arrived.shape[2] // 128, arrived.shape[1], 128), BF16
        ),
        compiler_params=pltpu.CompilerParams(vmem_limit_bytes=8 * 1024 * 1024),
        cost_estimate=pl.CostEstimate(flops=10**5, bytes_accessed=10**6, transcendentals=0),
    )(arrived, gain_qlat[None], gain_kvlat[None])


def two_terms(values):
    first = values.astype(BF16).astype(F32)
    return (first, (values - first).astype(BF16).astype(F32))


def attend_kernel(
    starts,
    base,
    packed,
    gain,
    query_turn,
    reach,
    w_query,
    w_key,
    w_value,
    key_turn,
    cache_rope,
    cache_lat,
    lat_out,
    rope_out,
    sent_out,
    q_lat,
    q_rot,
    k_rot,
    bias,
    numer,
    lat_rows,
    lat,
    rope,
    sent,
    lat_came,
    rope_came,
    lat_left,
    rope_left,
    sent_left,
):
    block = k_rot.shape[0]
    seq_count, pos_count, kvrank = cache_lat.shape
    qrank = w_query.shape[0]
    heads, lanes, _ = w_key.shape
    rope_dim = cache_rope.shape[1]
    half_dim = rope_dim // 2
    proposals = reach.shape[2]
    qkhead = lanes - rope_dim
    chunks = heads // 2
    scale = qkhead ** (-0.5)
    contract_last = (((1,), (1,)), ((), ()))
    contract_first = (((0,), (0,)), ((), ()))

    def coming(g):
        part = pl.ds(g * block, block)
        return (
            pltpu.make_async_copy(cache_lat.at[part], lat.at[part], lat_came.at[g]),
            pltpu.make_async_copy(cache_rope.at[part], rope.at[part], rope_came.at[g]),
        )

    def leaving(g):
        part = pl.ds(g * block, block)
        piece = pl.ds(g * block * chunks, block * chunks)
        return (
            pltpu.make_async_copy(lat.at[part], lat_out.at[part], lat_left.at[g]),
            pltpu.make_async_copy(rope.at[part], rope_out.at[part], rope_left.at[g]),
            pltpu.make_async_copy(sent.at[piece], sent_out.at[piece], sent_left.at[g]),
        )

    for g in range(seq_count // block):
        for copy in coming(g):
            copy.start()
    for c in range(lat_rows.shape[1] // 128):
        piece = packed[:, c]
        lat_rows[:, c * 128 : (c + 1) * 128] = piece.reshape(lat_rows.shape[0], 128)
    lane = lax.broadcasted_iota(jnp.int32, (1, lanes), 1)
    cosine = jnp.where(lane < rope_dim, query_turn[...], 0.0)
    sine = jnp.where(lane < rope_dim, pltpu.roll(query_turn[...], lanes - rope_dim, 1), 0.0)
    projected = jnp.dot(lat_rows[:, :qrank], w_query[...], preferred_element_type=F32)
    for h in range(heads):
        one = projected[:, h * lanes : (h + 1) * lanes]
        mean = jnp.sum(jnp.where(lane < qkhead, one * one, 0.0), axis=1, keepdims=True) / qkhead
        one = one * lax.rsqrt(mean + epsilon) * gain[...]
        at = pl.ds(h * proposals, proposals)
        moved = jnp.dot(one.astype(BF16), w_key[h], preferred_element_type=F32)
        q_lat[:, at, :] = moved.astype(BF16).reshape(seq_count, proposals, kvrank)
        turned = one * cosine + pltpu.roll(one, rope_dim, 1) * sine
        q_rot[:, at, :] = turned.astype(BF16).reshape(seq_count, proposals, lanes)

    @pl.loop(0, seq_count // block)
    def _(step):
        for copy in coming(step):
            copy.wait()
        for j in range(block):
            s = step * block + j
            rope32 = rope[s].astype(F32)
            low, high = rope32[:half_dim], rope32[half_dim:]
            key_cos, key_sin = key_turn[:half_dim], key_turn[half_dim:]
            k_rot[j, :half_dim] = (low * key_cos - high * key_sin).astype(BF16)
            k_rot[j, half_dim:] = (high * key_cos + low * key_sin).astype(BF16)
            offset = base[0] - starts[s]
            hit = (offset > -pos_count) & (offset < proposals)

            @pl.when(jnp.logical_not(hit))
            def _():
                bias[j] = jnp.full(bias.shape[1:], jnp.where(offset < 0, 0.0, HIDDEN), F32)

            @pl.when(hit)
            def _():
                rows = pl.ds(pl.multiple_of(s * proposals, proposals), proposals)
                down = lax.broadcasted_iota(jnp.int32, (pos_count, proposals), 0) + offset
                picked = down == lax.broadcasted_iota(jnp.int32, (pos_count, proposals), 1)
                across = lax.broadcasted_iota(jnp.int32, (proposals, pos_count), 1) + offset
                chosen = across == lax.broadcasted_iota(jnp.int32, (proposals, pos_count), 0)
                chosen = chosen.astype(F32).astype(BF16)
                along = lax.broadcasted_iota(jnp.int32, (1, pos_count), 1) + offset
                inside = (along >= 0) & (along < proposals)
                beneath = lax.broadcasted_iota(jnp.int32, (pos_count, 1), 0) + offset
                placed = jnp.dot(
                    picked.astype(F32).astype(BF16),
                    lat_rows[rows, qrank : qrank + kvrank],
                    preferred_element_type=F32,
                )
                lat[s] = jnp.where(
                    (beneath >= 0) & (beneath < proposals), placed, lat[s].astype(F32)
                ).astype(BF16)
                new_rope = lat_rows[rows, qrank + kvrank :].astype(F32)[:, :rope_dim]
                swapped = jnp.concatenate(
                    [new_rope[:, half_dim:], new_rope[:, :half_dim]], axis=1
                )
                turn = query_turn[rows, :]
                turned = (
                    new_rope * turn[:, :rope_dim] + swapped * turn[:, rope_dim : 2 * rope_dim]
                )
                put = lax.dot_general(
                    new_rope.astype(BF16), chosen, contract_first, preferred_element_type=F32
                )
                rope[s] = jnp.where(inside, put, rope32).astype(BF16)
                put = lax.dot_general(
                    turned.astype(BF16), chosen, contract_first, preferred_element_type=F32
                )
                k_rot[j] = jnp.where(inside, put, k_rot[j].astype(F32)).astype(BF16)
                seen = jnp.dot(reach[s], chosen, preferred_element_type=F32)
                shown = jnp.where((seen > 0.5) | (along < 0), 0.0, HIDDEN)
                for h in range(heads):
                    bias[j, h * proposals : (h + 1) * proposals, :] = shown

        for copy in leaving(step)[:2]:
            copy.start()
        for j in range(block):
            s = step * block + j
            keys = lat[s]
            score = lax.dot_general(
                q_lat[s], keys, contract_last, preferred_element_type=F32
            )
            score = score + jnp.dot(
                q_rot[s][:, :rope_dim], k_rot[j], preferred_element_type=F32
            )
            score = score * scale + bias[j]
            top = jnp.maximum(jnp.max(score, axis=1, keepdims=True), LOWEST)
            top_terms = two_terms(top)
            top = top_terms[0] + top_terms[1]
            weights = jnp.exp(score - top)
            total = jnp.sum(weights, axis=1, keepdims=True)
            numer[j] = jnp.dot(weights.astype(BF16), keys, preferred_element_type=F32)
            column = lax.broadcasted_iota(jnp.int32, (1, 128), 1)
            terms = jnp.zeros((heads * proposals, 128), F32)
            for k, term in enumerate((*top_terms, *two_terms(total))):
                terms = jnp.where(column == k, term, terms)
            extra = jnp.transpose(terms)[:4].astype(BF16)
            for c in range(chunks):
                sent[s * chunks + c, 8] = extra

        for h in range(heads):
            part = numer[:, pl.ds(h * proposals, proposals), :]
            part = part.reshape(block * proposals, kvrank)
            upper = part.astype(BF16)
            lower = (part - upper.astype(F32)).astype(BF16)
            both = jnp.dot(
                jnp.concatenate([upper, lower], axis=0), w_value[h], preferred_element_type=F32
            )
            value = (both[: block * proposals] + both[block * proposals :]).astype(BF16)
            for j in range(block):
                sent[
                    (step * block + j) * chunks + h // 2,
                    (h % 2) * 4 : (h % 2) * 4 + 4,
                ] = value[j * proposals : (j + 1) * proposals].reshape(4, 4, 128)
        leaving(step)[2].start()

    for g in range(seq_count // block):
        for copy in leaving(g):
            copy.wait()


def attend(starts, base, packed, gain, query_turn, reach, weights, key_turn, cache_rope, cache_lat):
    w_query, w_key, w_value = weights
    seq_count, pos_count, kvrank = cache_lat.shape
    rope_dim = cache_rope.shape[1]
    heads, lanes, _ = w_key.shape
    qrank = w_query.shape[0]
    proposals = reach.shape[2]
    rows = heads * proposals
    block = 16
    whole = pl.BlockSpec(memory_space=pltpu.VMEM)
    smem = pl.BlockSpec(memory_space=pltpu.SMEM)
    outside = pl.BlockSpec(memory_space=pltpu.HBM)
    sent_shape = (seq_count * heads // 2, 9, 4, w_value.shape[2])
    groups = seq_count // block
    return pl.pallas_call(
        attend_kernel,
        in_specs=[smem, smem, *[whole] * 8, outside, outside],
        out_specs=[outside] * 3,
        out_shape=[
            pltpu.HBM(cache_lat.shape, BF16),
            pltpu.HBM(cache_rope.shape, BF16),
            pltpu.HBM(sent_shape, BF16),
        ],
        scratch_shapes=[
            pltpu.VMEM((seq_count, rows, kvrank), BF16),
            pltpu.VMEM((seq_count, rows, lanes), BF16),
            pltpu.VMEM((block, rope_dim, pos_count), BF16),
            pltpu.VMEM((block, rows, pos_count), F32),
            pltpu.VMEM((block, rows, kvrank), F32),
            pltpu.VMEM((seq_count * proposals, qrank + kvrank + 128), BF16),
            pltpu.VMEM(cache_lat.shape, BF16),
            pltpu.VMEM(cache_rope.shape, BF16),
            pltpu.VMEM(sent_shape, BF16),
            *[pltpu.SemaphoreType.DMA((groups,))] * 5,
        ],
        compiler_params=pltpu.CompilerParams(vmem_limit_bytes=50 * 1024 * 1024),
        cost_estimate=pl.CostEstimate(
            flops=10**9, bytes_accessed=8 * 10**6, transcendentals=10**6
        ),
    )(starts, base, packed, gain, query_turn, reach, *weights, key_turn, cache_rope, cache_lat)


def project_kernel(heads_in, w_out, result):
    seq_count, heads, proposals, vhead = heads_in.shape
    total = jnp.zeros(result.shape, F32)
    for h in range(heads):
        total += jnp.dot(
            heads_in[:, h].reshape(seq_count * proposals, vhead),
            w_out[:, h * vhead : (h + 1) * vhead].T,
            preferred_element_type=F32,
        )
    result[...] = total


def project(heads_in, w_out):
    seq_count, heads, proposals, vhead = heads_in.shape
    return pl.pallas_call(
        project_kernel,
        out_shape=jax.ShapeDtypeStruct((seq_count * proposals, w_out.shape[0]), F32),
        in_specs=[pl.BlockSpec(memory_space=pltpu.VMEM)] * 2,
        out_specs=pl.BlockSpec(memory_space=pltpu.VMEM),
        compiler_params=pltpu.CompilerParams(vmem_limit_bytes=8 * 1024 * 1024),
        cost_estimate=pl.CostEstimate(
            flops=2 * 10**7, bytes_accessed=6 * 10**5, transcendentals=0
        ),
    )(heads_in, w_out)


def local(
    tokens,
    gain_in,
    w_qdown,
    w_kvdown,
    w_ropek,
    gain_qlat,
    gain_kvlat,
    w_qup,
    gain_q,
    w_ukey,
    w_uval,
    w_out,
    gain_out,
    cache_lat,
    cache_rope,
    parents,
    lengths,
    accepted,
):
    seq_count, proposals, local_width = tokens.shape
    rows = seq_count * proposals
    owners = lax.axis_size(KV)
    full_width = local_width * lax.axis_size(KV_TP)
    qrank, heads_here, qkhead = w_qup.shape
    kvrank, _, nope_dim = w_ukey.shape
    vhead = w_uval.shape[2]
    rope_dim = cache_rope.shape[1]
    half_dim = rope_dim // 2

    half = rows // lax.axis_size("tp")
    inputs = gather_inputs(
        lax.axis_index(KV_TP)[None], tokens, gain_in, w_qdown, w_kvdown, w_ropek
    )
    inputs = lax.all_gather(inputs, "tp", axis=0, tiled=True)
    own_rows = lax.dynamic_slice_in_dim(inputs, lax.axis_index("tp") * half, half, 1)
    partial_rows = lax.dot_general(
        own_rows, inputs[:, rows:], (((0,), (0,)), ((), ())), preferred_element_type=F32
    )
    arrived = exchange(partial_rows.reshape(owners, half // owners, -1), KV)
    everyone = exchange(latents(arrived, full_width, gain_qlat, gain_kvlat), KV)
    everyone = lax.all_gather(everyone, "tp", axis=0, tiled=True)
    reaches, depths = ancestry(parents)
    starts = lengths + accepted
    angles = rope_angles(starts[:, None] + depths, half_dim).reshape(rows, half_dim)
    cosine, sine = jnp.cos(angles), jnp.sin(angles)
    lanes = qkhead + rope_dim
    pos_count = cache_lat.shape[1]
    base = lax.axis_index(KV) * pos_count
    slot_angles = rope_angles(base + jnp.arange(pos_count, dtype=jnp.int32), half_dim).T
    query_turn = jnp.pad(
        jnp.concatenate([cosine, cosine, -sine, sine], axis=1),
        ((0, 0), (0, lanes - 2 * rope_dim)),
    )
    key_turn = jnp.concatenate([jnp.cos(slot_angles), jnp.sin(slot_angles)], axis=0)

    def arranged(values):
        nope, low, high = jnp.split(values, [nope_dim, nope_dim + half_dim], axis=-1)
        return jnp.concatenate([low, high, nope, high, low], axis=-1)

    weights = (
        arranged(w_qup).reshape(qrank, heads_here * lanes),
        jnp.pad(jnp.transpose(w_ukey, (1, 2, 0)), ((0, 0), (rope_dim, rope_dim), (0, 0))),
        jnp.transpose(w_uval, (1, 0, 2)),
    )
    lat_out, rope_out, sent = attend(
        starts,
        base[None],
        everyone,
        arranged(gain_q)[None],
        query_turn,
        reaches.astype(BF16),
        weights,
        key_turn,
        cache_rope,
        cache_lat,
    )
    arrived = exchange(sent, KV).astype(F32)
    group = 2 * proposals
    chunk = lax.rem(lax.axis_index(KV), heads_here // 2)
    extras = lax.dynamic_slice_in_dim(arrived[:, 8], chunk * group, group, 2)
    maxima = extras[:, 0] + extras[:, 1]
    factor = jnp.exp(maxima - jnp.max(maxima, axis=0))
    denom_all = jnp.sum(factor * (extras[:, 2] + extras[:, 3]), axis=0)
    values_all = jnp.sum(factor.reshape(owners, 8, 4, 1) * arrived[:, :8], axis=0)
    head_share = (values_all / denom_all.reshape(8, 4, 1)).astype(BF16).reshape(group, vhead)
    head_rows = from_everyone(head_share, KV)
    partial_out = project(head_rows.reshape(seq_count, heads_here, proposals, vhead), w_out.T)
    mixed = lax.all_gather(partial_out, "tp").sum(axis=0)
    local_squares = jnp.sum(mixed * mixed, axis=-1)
    norm_total = from_everyone(local_squares[None], KV).sum(axis=(0, 1))
    own = lax.dynamic_slice_in_dim(mixed, lax.axis_index("tp") * local_width, local_width, 1)
    result = own * lax.rsqrt(norm_total / full_width + epsilon)[:, None] * gain_out
    result = result.astype(BF16).reshape(seq_count, proposals, local_width)
    return (result, lat_out, rope_out)


def solution(mesh):
    torus = Mesh(
        mesh.devices.reshape(mesh.shape["dp"], 8, 8, mesh.shape["tp"]), ("dp", "kv_0", "kv_1", "tp")
    )
    return jax.shard_map(
        local,
        mesh=torus,
        in_specs=(
            P("dp", None, KV_TP),
            P(KV_TP),
            P(KV_TP, None),
            P(KV_TP, None),
            P(),
            P(),
            P(),
            P(None, "tp", None),
            P(),
            P(None, "tp", None),
            P(None, "tp", None),
            P("tp", KV),
            P(KV_TP),
            P("dp", KV, None),
            P("dp", None, KV),
            P("dp", None),
            P("dp"),
            P("dp"),
        ),
        out_specs=(P("dp", None, KV_TP), P("dp", KV, None), P("dp", None, KV)),
        check_vma=False,
    )
```

```python
import functools

import jax
import jax.numpy as jnp
from jax import lax
from jax.experimental import pallas as pl
from jax.experimental.pallas import tpu as pltpu
from jax.sharding import Mesh
from jax.sharding import PartitionSpec as P

KV_TP = ("kv_0", "kv_1", "tp")
KV = ("kv_0", "kv_1")

epsilon = 1e-06
F32 = jnp.float32
BF16 = jnp.bfloat16
LOWEST = -1e30
HIDDEN = -3e38


def exchange(parts, axes):
    return lax.all_to_all(parts, axes, split_axis=0, concat_axis=0, tiled=True)


def from_everyone(shard, axes):
    return exchange(jnp.broadcast_to(shard[None], (lax.axis_size(axes), *shard.shape)), axes)


def normed(values, gain_vec):
    return (
        values * lax.rsqrt(jnp.mean(values * values, axis=-1, keepdims=True) + epsilon) * gain_vec
    )


def rope_angles(position, half_dim):
    frequency = 10000.0 ** (-(jnp.arange(half_dim, dtype=jnp.float32) * 2.0) / (2 * half_dim))
    return position.astype(jnp.float32)[..., None] * frequency


def ancestry(parents):
    proposals = parents.shape[-1]
    step = (parents[..., :, None] == jnp.arange(proposals, dtype=jnp.int32)).astype(BF16)
    reaches = step + jnp.eye(proposals, dtype=BF16)
    covered = 2
    while covered < proposals:
        step = jnp.einsum("sij,sjk->sik", step, step, preferred_element_type=F32).astype(BF16)
        reaches = reaches + jnp.einsum(
            "sij,sjk->sik", reaches, step, preferred_element_type=F32
        ).astype(BF16)
        covered *= 2
    reaches = reaches.astype(F32)
    depths = (jnp.sum(reaches, axis=-1) - 1.0).astype(jnp.int32)
    return (reaches, depths)


def gather_kernel(index, tokens, gain, w_qdown, w_kvdown, rope_columns, out):
    width = tokens.shape[2]
    rows = tokens.shape[0] * tokens.shape[1]
    qrank, kvrank = w_qdown.shape[1], w_kvdown.shape[1]
    rope_dim, lanes = rope_columns.shape
    tok_rows = tokens[...].astype(F32).reshape(rows, width)
    scaled = (tok_rows * gain[...]).astype(BF16).astype(F32)
    out[:width, :rows] = jnp.transpose(scaled).astype(BF16)
    out[:width, rows : rows + qrank] = w_qdown[...]
    out[:width, rows + qrank : rows + qrank + kvrank] = w_kvdown[...]
    at = rows + qrank + kvrank
    shift = lax.rem(lanes - lax.rem(index[0] * width, lanes), lanes)
    turned = pltpu.roll(rope_columns[...].astype(F32), shift, 1)
    padded = jnp.concatenate([turned, jnp.zeros((lanes - rope_dim, lanes), F32)], axis=0)
    out[:width, at:] = jnp.transpose(padded)[:width].astype(BF16)
    flipped = jnp.transpose(tok_rows)
    squares = jnp.sum(flipped * flipped, axis=0, keepdims=True)
    row = lax.broadcasted_iota(jnp.int32, (width, rows), 0)
    terms = jnp.zeros((width, rows), F32)
    for k in range(3):
        term = squares.astype(BF16).astype(F32)
        terms = jnp.where(row == k, term, terms)
        squares = squares - term
    out[width:, :rows] = terms.astype(BF16)
    out[width:, rows:at] = jnp.zeros((width, at - rows), BF16)
    row = lax.broadcasted_iota(jnp.int32, (width, lanes), 0)
    lane = lax.broadcasted_iota(jnp.int32, (width, lanes), 1)
    out[width:, at:] = jnp.where((row < 3) & (lane == rope_dim), 1.0, 0.0).astype(BF16)


def gather_inputs(index, tokens, gain_in, w_qdown, w_kvdown, w_ropek):
    width = tokens.shape[2]
    rows = tokens.shape[0] * tokens.shape[1]
    lanes = 128
    whole = pl.BlockSpec(memory_space=pltpu.VMEM)
    shape = (2 * width, rows + w_qdown.shape[1] + w_kvdown.shape[1] + lanes)
    return pl.pallas_call(
        gather_kernel,
        grid_spec=pltpu.PrefetchScalarGridSpec(
            num_scalar_prefetch=1,
            grid=(1,),
            in_specs=[
                *[whole] * 4,
                pl.BlockSpec(
                    (w_ropek.shape[1], lanes), lambda g, index: (0, index[0] * width // lanes)
                ),
            ],
            out_specs=whole,
        ),
        out_shape=pltpu.VMEM(shape, BF16),
        cost_estimate=pl.CostEstimate(flops=10**5, bytes_accessed=10**5, transcendentals=0),
    )(index, tokens, gain_in[None], w_qdown, w_kvdown, w_ropek.T)


def latent_kernel(full_width, arrived, gain_qlat, gain_kvlat, out):
    qrank, kvrank = gain_qlat.shape[1], gain_kvlat.shape[1]
    summed = jnp.sum(arrived[...], axis=0)
    lanes = 128
    at = qrank + kvrank
    lane = lax.broadcasted_iota(jnp.int32, (1, lanes), 1)
    last = summed[:, at:]
    rope_dim = 32
    squares = jnp.sum(jnp.where(lane == rope_dim, last, 0.0), axis=1, keepdims=True)
    rescale = lax.rsqrt(squares / full_width + epsilon)
    share = jnp.concatenate(
        [
            normed(summed[:, :qrank] * rescale, gain_qlat[...]),
            normed(summed[:, qrank:at] * rescale, gain_kvlat[...]),
            jnp.where(lane < rope_dim, last * rescale, 0.0),
        ],
        axis=1,
    )
    for c in range(share.shape[1] // lanes):
        piece = share[:, c * lanes : (c + 1) * lanes].astype(BF16)
        out[:, c] = jnp.broadcast_to(piece[None], (out.shape[0], *piece.shape))


def latents(arrived, full_width, gain_qlat, gain_kvlat):
    owners = arrived.shape[0]
    return pl.pallas_call(
        functools.partial(latent_kernel, full_width),
        in_specs=[pl.BlockSpec(memory_space=pltpu.VMEM)] * 3,
        out_specs=pl.BlockSpec(memory_space=pltpu.VMEM),
        out_shape=jax.ShapeDtypeStruct(
            (owners, arrived.shape[2] // 128, arrived.shape[1], 128), BF16
        ),
        compiler_params=pltpu.CompilerParams(vmem_limit_bytes=8 * 1024 * 1024),
        cost_estimate=pl.CostEstimate(flops=10**5, bytes_accessed=10**6, transcendentals=0),
    )(arrived, gain_qlat[None], gain_kvlat[None])


def two_terms(values):
    first = values.astype(BF16).astype(F32)
    return (first, (values - first).astype(BF16).astype(F32))


def attend_kernel(
    starts,
    base,
    packed,
    gain,
    query_turn,
    reach,
    w_query,
    w_key,
    w_value,
    key_turn,
    cache_rope,
    cache_lat,
    lat_out,
    rope_out,
    sent_out,
    q_lat,
    q_rot,
    k_rot,
    bias,
    numer,
    lat_rows,
    lat,
    rope,
    sent,
    lat_came,
    rope_came,
    lat_left,
    rope_left,
    sent_left,
):
    block = k_rot.shape[0]
    seq_count, pos_count, kvrank = cache_lat.shape
    qrank = w_query.shape[0]
    heads, lanes, _ = w_key.shape
    rope_dim = cache_rope.shape[1]
    half_dim = rope_dim // 2
    proposals = reach.shape[2]
    qkhead = lanes - rope_dim
    chunks = heads // 2
    scale = qkhead ** (-0.5)
    contract_last = (((1,), (1,)), ((), ()))
    contract_first = (((0,), (0,)), ((), ()))

    def coming(g):
        part = pl.ds(g * block, block)
        return (
            pltpu.make_async_copy(cache_lat.at[part], lat.at[part], lat_came.at[g]),
            pltpu.make_async_copy(cache_rope.at[part], rope.at[part], rope_came.at[g]),
        )

    def leaving(g):
        part = pl.ds(g * block, block)
        return (
            pltpu.make_async_copy(lat.at[part], lat_out.at[part], lat_left.at[g]),
            pltpu.make_async_copy(rope.at[part], rope_out.at[part], rope_left.at[g]),
            *(
                pltpu.make_async_copy(
                    sent.at[part, c], sent_out.at[part, c], sent_left.at[g, c]
                )
                for c in range(chunks)
            ),
        )

    for g in range(seq_count // block):
        for copy in coming(g):
            copy.start()
    for c in range(lat_rows.shape[1] // 128):
        piece = packed[:, c]
        lat_rows[:, c * 128 : (c + 1) * 128] = piece.reshape(lat_rows.shape[0], 128)
    lane = lax.broadcasted_iota(jnp.int32, (1, lanes), 1)
    cosine = jnp.where(lane < rope_dim, query_turn[...], 0.0)
    sine = jnp.where(lane < rope_dim, pltpu.roll(query_turn[...], lanes - rope_dim, 1), 0.0)
    projected = jnp.dot(lat_rows[:, :qrank], w_query[...], preferred_element_type=F32)
    for h in range(heads):
        one = projected[:, h * lanes : (h + 1) * lanes]
        mean = jnp.sum(jnp.where(lane < qkhead, one * one, 0.0), axis=1, keepdims=True) / qkhead
        one = one * lax.rsqrt(mean + epsilon) * gain[...]
        at = pl.ds(h * proposals, proposals)
        moved = jnp.dot(one.astype(BF16), w_key[h], preferred_element_type=F32)
        q_lat[:, at, :] = moved.astype(BF16).reshape(seq_count, proposals, kvrank)
        turned = one * cosine + pltpu.roll(one, rope_dim, 1) * sine
        q_rot[:, at, :] = turned.astype(BF16).reshape(seq_count, proposals, lanes)

    @pl.loop(0, seq_count // block)
    def _(step):
        for copy in coming(step):
            copy.wait()
        for j in range(block):
            s = step * block + j
            rope32 = rope[s].astype(F32)
            low, high = rope32[:half_dim], rope32[half_dim:]
            key_cos, key_sin = key_turn[:half_dim], key_turn[half_dim:]
            k_rot[j, :half_dim] = (low * key_cos - high * key_sin).astype(BF16)
            k_rot[j, half_dim:] = (high * key_cos + low * key_sin).astype(BF16)
            offset = base[0] - starts[s]
            hit = (offset > -pos_count) & (offset < proposals)

            @pl.when(jnp.logical_not(hit))
            def _():
                bias[j] = jnp.full(bias.shape[1:], jnp.where(offset < 0, 0.0, HIDDEN), F32)

            @pl.when(hit)
            def _():
                rows = pl.ds(pl.multiple_of(s * proposals, proposals), proposals)
                down = lax.broadcasted_iota(jnp.int32, (pos_count, proposals), 0) + offset
                picked = down == lax.broadcasted_iota(jnp.int32, (pos_count, proposals), 1)
                across = lax.broadcasted_iota(jnp.int32, (proposals, pos_count), 1) + offset
                chosen = across == lax.broadcasted_iota(jnp.int32, (proposals, pos_count), 0)
                chosen = chosen.astype(F32).astype(BF16)
                along = lax.broadcasted_iota(jnp.int32, (1, pos_count), 1) + offset
                inside = (along >= 0) & (along < proposals)
                beneath = lax.broadcasted_iota(jnp.int32, (pos_count, 1), 0) + offset
                placed = jnp.dot(
                    picked.astype(F32).astype(BF16),
                    lat_rows[rows, qrank : qrank + kvrank],
                    preferred_element_type=F32,
                )
                lat[s] = jnp.where(
                    (beneath >= 0) & (beneath < proposals), placed, lat[s].astype(F32)
                ).astype(BF16)
                new_rope = lat_rows[rows, qrank + kvrank :].astype(F32)[:, :rope_dim]
                swapped = jnp.concatenate(
                    [new_rope[:, half_dim:], new_rope[:, :half_dim]], axis=1
                )
                turn = query_turn[rows, :]
                turned = (
                    new_rope * turn[:, :rope_dim] + swapped * turn[:, rope_dim : 2 * rope_dim]
                )
                put = lax.dot_general(
                    new_rope.astype(BF16), chosen, contract_first, preferred_element_type=F32
                )
                rope[s] = jnp.where(inside, put, rope32).astype(BF16)
                put = lax.dot_general(
                    turned.astype(BF16), chosen, contract_first, preferred_element_type=F32
                )
                k_rot[j] = jnp.where(inside, put, k_rot[j].astype(F32)).astype(BF16)
                seen = jnp.dot(reach[s], chosen, preferred_element_type=F32)
                shown = jnp.where((seen > 0.5) | (along < 0), 0.0, HIDDEN)
                for h in range(heads):
                    bias[j, h * proposals : (h + 1) * proposals, :] = shown

        for copy in leaving(step)[:2]:
            copy.start()
        for j in range(block):
            s = step * block + j
            keys = lat[s]
            score = lax.dot_general(
                q_lat[s], keys, contract_last, preferred_element_type=F32
            )
            score = score + jnp.dot(
                q_rot[s][:, :rope_dim], k_rot[j], preferred_element_type=F32
            )
            score = score * scale + bias[j]
            top = jnp.maximum(jnp.max(score, axis=1, keepdims=True), LOWEST)
            top_terms = two_terms(top)
            top = top_terms[0] + top_terms[1]
            weights = jnp.exp(score - top)
            total = jnp.sum(weights, axis=1, keepdims=True)
            numer[j] = jnp.dot(weights.astype(BF16), keys, preferred_element_type=F32)
            column = lax.broadcasted_iota(jnp.int32, (1, 128), 1)
            terms = jnp.zeros((heads * proposals, 128), F32)
            for k, term in enumerate((*top_terms, *two_terms(total))):
                terms = jnp.where(column == k, term, terms)
            extra = jnp.transpose(terms)[:4].astype(BF16)
            for c in range(chunks):
                sent[s, c, 8] = extra

        for h in range(heads):
            part = numer[:, pl.ds(h * proposals, proposals), :]
            part = part.reshape(block * proposals, kvrank)
            upper = part.astype(BF16)
            lower = (part - upper.astype(F32)).astype(BF16)
            both = jnp.dot(
                jnp.concatenate([upper, lower], axis=0), w_value[h], preferred_element_type=F32
            )
            value = (both[: block * proposals] + both[block * proposals :]).astype(BF16)
            for j in range(block):
                sent[step * block + j, h // 2, (h % 2) * 4 : (h % 2) * 4 + 4] = value[
                    j * proposals : (j + 1) * proposals
                ].reshape(4, 4, 128)
            if h % 2 == 1:
                leaving(step)[2 + h // 2].start()

    for g in range(seq_count // block):
        for copy in leaving(g):
            copy.wait()


def attend(starts, base, packed, gain, query_turn, reach, weights, key_turn, cache_rope, cache_lat):
    w_query, w_key, w_value = weights
    seq_count, pos_count, kvrank = cache_lat.shape
    rope_dim = cache_rope.shape[1]
    heads, lanes, _ = w_key.shape
    qrank = w_query.shape[0]
    proposals = reach.shape[2]
    rows = heads * proposals
    block = 16
    whole = pl.BlockSpec(memory_space=pltpu.VMEM)
    smem = pl.BlockSpec(memory_space=pltpu.SMEM)
    outside = pl.BlockSpec(memory_space=pltpu.HBM)
    sent_shape = (seq_count, heads // 2, 9, 4, w_value.shape[2])
    groups = seq_count // block
    return pl.pallas_call(
        attend_kernel,
        in_specs=[smem, smem, *[whole] * 8, outside, outside],
        out_specs=[outside] * 3,
        out_shape=[
            pltpu.HBM(cache_lat.shape, BF16),
            pltpu.HBM(cache_rope.shape, BF16),
            pltpu.HBM(sent_shape, BF16),
        ],
        scratch_shapes=[
            pltpu.VMEM((seq_count, rows, kvrank), BF16),
            pltpu.VMEM((seq_count, rows, lanes), BF16),
            pltpu.VMEM((block, rope_dim, pos_count), BF16),
            pltpu.VMEM((block, rows, pos_count), F32),
            pltpu.VMEM((block, rows, kvrank), F32),
            pltpu.VMEM((seq_count * proposals, qrank + kvrank + 128), BF16),
            pltpu.VMEM(cache_lat.shape, BF16),
            pltpu.VMEM(cache_rope.shape, BF16),
            pltpu.VMEM(sent_shape, BF16),
            *[pltpu.SemaphoreType.DMA((groups,))] * 4,
            pltpu.SemaphoreType.DMA((groups, heads // 2)),
        ],
        compiler_params=pltpu.CompilerParams(vmem_limit_bytes=50 * 1024 * 1024),
        cost_estimate=pl.CostEstimate(
            flops=10**9, bytes_accessed=8 * 10**6, transcendentals=10**6
        ),
    )(starts, base, packed, gain, query_turn, reach, *weights, key_turn, cache_rope, cache_lat)


def project_kernel(heads_in, w_out, result):
    seq_count, heads, proposals, vhead = heads_in.shape
    total = jnp.zeros(result.shape, F32)
    for h in range(heads):
        total += jnp.dot(
            heads_in[:, h].reshape(seq_count * proposals, vhead),
            w_out[:, h * vhead : (h + 1) * vhead].T,
            preferred_element_type=F32,
        )
    result[...] = total


def project(heads_in, w_out):
    seq_count, heads, proposals, vhead = heads_in.shape
    return pl.pallas_call(
        project_kernel,
        out_shape=jax.ShapeDtypeStruct((seq_count * proposals, w_out.shape[0]), F32),
        in_specs=[pl.BlockSpec(memory_space=pltpu.VMEM)] * 2,
        out_specs=pl.BlockSpec(memory_space=pltpu.VMEM),
        compiler_params=pltpu.CompilerParams(vmem_limit_bytes=8 * 1024 * 1024),
        cost_estimate=pl.CostEstimate(
            flops=2 * 10**7, bytes_accessed=6 * 10**5, transcendentals=0
        ),
    )(heads_in, w_out)


def local(
    tokens,
    gain_in,
    w_qdown,
    w_kvdown,
    w_ropek,
    gain_qlat,
    gain_kvlat,
    w_qup,
    gain_q,
    w_ukey,
    w_uval,
    w_out,
    gain_out,
    cache_lat,
    cache_rope,
    parents,
    lengths,
    accepted,
):
    seq_count, proposals, local_width = tokens.shape
    rows = seq_count * proposals
    owners = lax.axis_size(KV)
    full_width = local_width * lax.axis_size(KV_TP)
    qrank, heads_here, qkhead = w_qup.shape
    kvrank, _, nope_dim = w_ukey.shape
    vhead = w_uval.shape[2]
    rope_dim = cache_rope.shape[1]
    half_dim = rope_dim // 2

    half = rows // lax.axis_size("tp")
    inputs = gather_inputs(
        lax.axis_index(KV_TP)[None], tokens, gain_in, w_qdown, w_kvdown, w_ropek
    )
    inputs = lax.all_gather(inputs, "tp", axis=0, tiled=True)
    own_rows = lax.dynamic_slice_in_dim(inputs, lax.axis_index("tp") * half, half, 1)
    partial_rows = lax.dot_general(
        own_rows, inputs[:, rows:], (((0,), (0,)), ((), ())), preferred_element_type=F32
    )
    arrived = exchange(partial_rows.reshape(owners, half // owners, -1), KV)
    everyone = exchange(latents(arrived, full_width, gain_qlat, gain_kvlat), KV)
    everyone = lax.all_gather(everyone, "tp", axis=0, tiled=True)
    reaches, depths = ancestry(parents)
    starts = lengths + accepted
    angles = rope_angles(starts[:, None] + depths, half_dim).reshape(rows, half_dim)
    cosine, sine = jnp.cos(angles), jnp.sin(angles)
    lanes = qkhead + rope_dim
    pos_count = cache_lat.shape[1]
    base = lax.axis_index(KV) * pos_count
    slot_angles = rope_angles(base + jnp.arange(pos_count, dtype=jnp.int32), half_dim).T
    query_turn = jnp.pad(
        jnp.concatenate([cosine, cosine, -sine, sine], axis=1),
        ((0, 0), (0, lanes - 2 * rope_dim)),
    )
    key_turn = jnp.concatenate([jnp.cos(slot_angles), jnp.sin(slot_angles)], axis=0)

    def arranged(values):
        nope, low, high = jnp.split(values, [nope_dim, nope_dim + half_dim], axis=-1)
        return jnp.concatenate([low, high, nope, high, low], axis=-1)

    weights = (
        arranged(w_qup).reshape(qrank, heads_here * lanes),
        jnp.pad(jnp.transpose(w_ukey, (1, 2, 0)), ((0, 0), (rope_dim, rope_dim), (0, 0))),
        jnp.transpose(w_uval, (1, 0, 2)),
    )
    lat_out, rope_out, sent = attend(
        starts,
        base[None],
        everyone,
        arranged(gain_q)[None],
        query_turn,
        reaches.astype(BF16),
        weights,
        key_turn,
        cache_rope,
        cache_lat,
    )
    arrived = exchange(sent.reshape(owners, *sent.shape[2:]), KV).astype(F32)
    group = 2 * proposals
    chunk = lax.rem(lax.axis_index(KV), heads_here // 2)
    extras = lax.dynamic_slice_in_dim(arrived[:, 8], chunk * group, group, 2)
    maxima = extras[:, 0] + extras[:, 1]
    factor = jnp.exp(maxima - jnp.max(maxima, axis=0))
    denom_all = jnp.sum(factor * (extras[:, 2] + extras[:, 3]), axis=0)
    values_all = jnp.sum(factor.reshape(owners, 8, 4, 1) * arrived[:, :8], axis=0)
    head_share = (values_all / denom_all.reshape(8, 4, 1)).astype(BF16).reshape(group, vhead)
    head_rows = from_everyone(head_share, KV)
    partial_out = project(head_rows.reshape(seq_count, heads_here, proposals, vhead), w_out.T)
    mixed = lax.all_gather(partial_out, "tp").sum(axis=0)
    local_squares = jnp.sum(mixed * mixed, axis=-1)
    norm_total = from_everyone(local_squares[None], KV).sum(axis=(0, 1))
    own = lax.dynamic_slice_in_dim(mixed, lax.axis_index("tp") * local_width, local_width, 1)
    result = own * lax.rsqrt(norm_total / full_width + epsilon)[:, None] * gain_out
    result = result.astype(BF16).reshape(seq_count, proposals, local_width)
    return (result, lat_out, rope_out)


def solution(mesh):
    torus = Mesh(
        mesh.devices.reshape(mesh.shape["dp"], 8, 8, mesh.shape["tp"]), ("dp", "kv_0", "kv_1", "tp")
    )
    return jax.shard_map(
        local,
        mesh=torus,
        in_specs=(
            P("dp", None, KV_TP),
            P(KV_TP),
            P(KV_TP, None),
            P(KV_TP, None),
            P(),
            P(),
            P(),
            P(None, "tp", None),
            P(),
            P(None, "tp", None),
            P(None, "tp", None),
            P("tp", KV),
            P(KV_TP),
            P("dp", KV, None),
            P("dp", None, KV),
            P("dp", None),
            P("dp"),
            P("dp"),
        ),
        out_specs=(P("dp", None, KV_TP), P("dp", KV, None), P("dp", None, KV)),
        check_vma=False,
    )
```
